256 devices in a mesh: ep: 64 (over z, x, core), tp: 4 (over y).
Axes of the slice: x: 4, y: 4, z: 8, core: 2. Of those that a mesh axis runs over, the one named last changes fastest.
Arguments:
- queries: bfloat16 [16384, 1024], P('ep', 'tp'), may hold values from -192 to 192
- keys_values: bfloat16 [16384, 512], P('ep', 'tp'), may hold values from -192 to 192
- log_gate_cum: float32 [16, 16384], P('tp'), as said below
- mix_weight: bfloat16 [1024, 2048], P('tp'), may hold values from -0.1875 to 0.1875
- mix_gain: float32 [2048], replicated, may hold values from 0.1 to 1.9
- moe_in: bfloat16 [49152, 2048], P(('ep', 'tp')), may hold values from -6 to 6
- moe_gain: float32 [2048], replicated, may hold values from 0.1 to 1.9
- routes: int32 [49152, 2], P(('ep', 'tp')), may hold values from 0 to 63, all different within a row; in each aligned block of 192 rows (0 to 191, 192 to 383, ...) at most 9 rows name the same one
- route_weight: float32 [49152, 2], P(('ep', 'tp')), may hold values from 0.25 to 2
- expert_gate: bfloat16 [64, 2048, 1024], P('ep', None, 'tp'), may hold values from -0.125 to 0.125
- expert_up: bfloat16 [64, 2048, 1024], P('ep', None, 'tp'), may hold values from -0.125 to 0.125
- expert_down: bfloat16 [64, 1024, 2048], P('ep', 'tp'), may hold values from -0.1875 to 0.1875
Outputs:
- mix_result: bfloat16 [16384, 2048], P(('ep', 'tp'))
- moe_result: bfloat16 [49152, 2048], P(('ep', 'tp'))
The draws below stay inside these ranges and needn't reach their ends.
Inputs may be any that keep to these rules, and one draw needn't show every extreme that they name: `log_gate_cum`: along positions each head's values never rise. `routes`: each row names 2 different experts. Among the rows of one device no expert is named more than 9 times, and in every draw some device names some expert exactly 9 times.
All inputs are finite; a program needn't handle non-finite values.
Results may differ from the reference program's by a relative error of at most 0.013.
Values may be sent and summed in bfloat16 or wider, within the bound.
No kernel may reach another device: no remote copies, remote signals or barrier semaphores. Data moves between devices by JAX's collectives and lax.ppermute only.
A program may use at most 128 MiB of HBM per device.

```python
import math
import jax
import jax.numpy as jnp
import numpy as np
from jax import lax

D = 2048
ASKING_ATTENDERS = 16
KV_HEADS = 4
HEAD = 64
FF = 1024
TOPK = 2
TOK_EP = 256
TOK_M = 192
CONTEXT_SPAN = 16384
EXPERTS = 64
CAP = 9
TOKENS_M = 49152
N_EP = 64
N_TP = 4


def attention_pair(key):
    queries = jnp.clip(jax.random.normal(jax.random.fold_in(key, 31), (CONTEXT_SPAN, ASKING_ATTENDERS * HEAD), jnp.float32), -4.5, 4.5)
    paired = jnp.clip(jax.random.normal(jax.random.fold_in(key, 32), (CONTEXT_SPAN, KV_HEADS, 2, HEAD), jnp.float32), -4.5, 4.5)
    return (queries, paired.reshape(CONTEXT_SPAN, KV_HEADS * 2 * HEAD))


def draw_queries(key, part):
    return attention_pair(key)[0].astype(jnp.bfloat16)


def draw_keys_values(key, part):
    return attention_pair(key)[1].astype(jnp.bfloat16)


def draw_log_gate_cum(key, part):
    attender_ordinal = jnp.arange(ASKING_ATTENDERS, dtype=jnp.int32)
    ranking = jax.random.permutation(jax.random.fold_in(key, 41), ASKING_ATTENDERS)
    fast_count = ASKING_ATTENDERS // 2
    is_fast = ranking < fast_count
    fast_rate = jnp.exp(jax.random.uniform(jax.random.fold_in(key, 42), (ASKING_ATTENDERS,), jnp.float32, math.log(0.01), math.log(1.0 / 30.0)))
    slow_rate = jnp.exp(jax.random.uniform(jax.random.fold_in(key, 43), (ASKING_ATTENDERS,), jnp.float32, math.log(0.3), 0.0)) / CONTEXT_SPAN
    rate = jnp.where(is_fast, fast_rate, slow_rate)[:, None]
    block_factor = jnp.exp(jax.random.uniform(jax.random.fold_in(key, 44), (ASKING_ATTENDERS, N_EP), jnp.float32, math.log(0.5), math.log(2.0)))
    block_factor = jnp.repeat(block_factor, TOK_EP, axis=1)
    roughness = jax.random.uniform(jax.random.fold_in(key, 45), (ASKING_ATTENDERS, CONTEXT_SPAN), jnp.float32, 0.3, 1.7)
    doubling_rounds = -rate * block_factor * roughness
    span_offset = jax.random.randint(jax.random.fold_in(key, 46), (ASKING_ATTENDERS, 3), 0, CONTEXT_SPAN)
    span_extent = jax.random.uniform(jax.random.fold_in(key, 47), (ASKING_ATTENDERS, 3), jnp.float32, 0.22, 0.5)
    doubling_rounds = doubling_rounds.at[attender_ordinal[:, None], span_offset].add(-span_extent)
    return jnp.cumsum(doubling_rounds, axis=1)


def steps_of(key, dims, shards, low, top_value):
    factor_of, own = 1.0, jax.random.fold_in(key, 6)
    for position, shards_of in shards:
        heights = jnp.exp(jax.random.uniform(jax.random.fold_in(own, position), (shards_of,), jnp.float32, low / len(shards), top_value / len(shards)))
        factor_of = factor_of * jnp.repeat(heights, dims[position] // shards_of).reshape([-1 if axis == position else 1 for axis in range(len(dims))])
    return factor_of


def assign_block(stream_key, own, number, rows, amount, top, most, slope):
    order = jax.random.permutation(stream_key, amount)
    crowded, ordinary = shares(amount, rows * top, most, slope, True), shares(amount, rows * top, most, slope, False)
    places = jnp.arange(amount)

    def named(sizes, turn):
        used = int((sizes > 0).sum())
        fixed = max(1, used // 4)
        shifted = fixed + (places - fixed + turn * (used - fixed)) % max(1, amount - fixed)
        return jnp.zeros((amount,), jnp.int32).at[order[jnp.where(places < fixed, places, shifted)]].set(jnp.asarray(sizes, jnp.int32))

    sizes = jnp.where(number % 4 == 0, named(crowded, number // 4), named(ordinary, number - number // 4 - 1))
    mixed = jax.random.permutation(jax.random.fold_in(own, 3), amount)
    source_of, sink = mixed[0:amount // 2 * 2:2], mixed[1:amount // 2 * 2:2]
    margin = jnp.minimum(sizes[source_of] - 1, most - sizes[sink]) // 2
    margin = jnp.where((source_of == order[0]) | (sink == order[0]) | (sizes[sink] == 0), 0, jnp.maximum(margin, 0))
    shifted = jax.random.randint(jax.random.fold_in(own, 4), (amount // 2,), 0, 1 << 20) % (margin + 1)
    sizes = sizes.at[source_of].add(-shifted).at[sink].add(shifted)
    items = jnp.searchsorted(jnp.cumsum(sizes), jnp.arange(rows * top), side="right").astype(jnp.int32)
    grid = items.reshape(top, rows).T
    grid = grid[jax.random.permutation(jax.random.fold_in(own, 1), rows)]
    turn = jax.random.randint(jax.random.fold_in(own, 2), (rows, 1), 0, top)
    return jnp.take_along_axis(grid, (jnp.arange(top)[None, :] + turn) % top, axis=1)


def shares(number_of, total, limit, slope, full):
    weights = [(1 << 20) // math.isqrt(grade ** slope) + 1 for grade in range(1, number_of + 1)]
    largest = limit if full else min(limit, max(-(-total // number_of), total * weights[0] // sum(weights)))
    least = 1 if total - largest >= number_of - 1 else 0
    given, spare = [largest] + [least] * (number_of - 1), total - largest - least * (number_of - 1)
    while spare > 0:
        movable = [i for i in range(1, number_of) if given[i] < largest] or [i for i in range(1, number_of) if given[i] < limit]
        pool, budget = sum([weights[i] for i in movable]), spare
        for i in movable:
            extra = min(limit - given[i], max(1, budget * weights[i] // pool), spare)
            given[i] = given[i] + extra
            spare = spare - extra
    return np.array(given)


def gaussian(rng, shape, deviation, limit, pieces=(), kind=jnp.bfloat16):
    values = deviation * jax.random.normal(rng, shape, jnp.float32)
    if pieces:
        values = values * steps_of(rng, shape, pieces, -0.22, 0.18)
    return jnp.clip(values, -limit, limit).astype(kind)


def setup_inputs(seed: int = 0) -> dict:
    seeds = jax.random.split(jax.random.key(seed), 13)
    queries = draw_queries(jax.random.fold_in(seeds[12], 71), 0)
    keys_values = draw_keys_values(jax.random.fold_in(seeds[12], 71), 0)
    log_gate_cum = draw_log_gate_cum(jax.random.fold_in(seeds[12], 71), 0)
    mix_weight = gaussian(seeds[3], (ASKING_ATTENDERS * HEAD, D), (ASKING_ATTENDERS * HEAD) ** -0.5, 0.1875, ((0, 4),))
    mix_gain = jnp.clip(1.0 + 0.18 * jax.random.normal(seeds[4], (D,), jnp.float32), 0.1, 1.9)
    moe_in = gaussian(seeds[5], (TOKENS_M, D), 1.0, 6.0, ((0, 256),))
    moe_gain = jnp.clip(1.0 + 0.18 * jax.random.normal(seeds[6], (D,), jnp.float32), 0.1, 1.9)
    routes_keys = jax.random.split(jax.random.fold_in(seeds[7], 1), TOKENS_M // TOK_M)
    routes_turns = jax.random.permutation(jax.random.fold_in(seeds[7], 3), TOKENS_M // TOK_M)
    routes = jax.vmap(lambda own, number: assign_block(jax.random.fold_in(seeds[7], 2), own, number, TOK_M, EXPERTS, TOPK, CAP, 2))(routes_keys, routes_turns).reshape((TOKENS_M, TOPK))
    route_weight = jnp.clip(jnp.exp(math.log(2.0) - 2.0794415 * jax.random.uniform(seeds[8], (TOKENS_M, TOPK), jnp.float32) ** steps_of(seeds[8], (TOKENS_M, TOPK), ((0, 256),), -0.2, 0.2)), 0.25, 2.0)
    expert_gate = gaussian(seeds[9], (EXPERTS, D, FF), D ** -0.5, 0.125, ((0, 64), (2, 4)))
    expert_up = gaussian(seeds[10], (EXPERTS, D, FF), D ** -0.5, 0.125, ((0, 64), (2, 4)))
    expert_down = gaussian(seeds[11], (EXPERTS, FF, D), FF ** -0.5, 0.1875, ((0, 64), (1, 4)))
    return dict(queries=queries, keys_values=keys_values, log_gate_cum=log_gate_cum, mix_weight=mix_weight, mix_gain=mix_gain, moe_in=moe_in, moe_gain=moe_gain, routes=routes, route_weight=route_weight, expert_gate=expert_gate, expert_up=expert_up, expert_down=expert_down)


EPSILON = 1e-06

def rms_scale(values, gain):
    widened = values.astype(jnp.float32)
    return widened * lax.rsqrt(lax.optimization_barrier(jnp.mean(widened * widened, axis=-1, keepdims=True)) + EPSILON) * gain

def attend_reference(queries, keys_values, log_gate_cum):
    seq_len = queries.shape[0]
    group_size = ASKING_ATTENDERS // KV_HEADS
    block_rows = math.gcd(seq_len, 256)
    paired = keys_values.reshape(seq_len, KV_HEADS, 2, HEAD).astype(jnp.float32)
    key_part = paired[:, :, 0]
    value_part = paired[:, :, 1]
    gates = log_gate_cum.reshape(KV_HEADS, group_size, seq_len)
    key_pos = jnp.arange(seq_len, dtype=jnp.int32)

    def one_block(block_index):
        first_row = block_index * block_rows
        query_block = lax.dynamic_slice_in_dim(queries, first_row, block_rows, 0)
        query_block = query_block.reshape(block_rows, KV_HEADS, group_size, HEAD).astype(jnp.float32)
        scores = jnp.einsum('tgrd,ngd->grtn', query_block, key_part) * HEAD ** (-0.5)
        query_gate = lax.dynamic_slice_in_dim(gates, first_row, block_rows, 2)
        scores = scores + query_gate[..., None] - gates[:, :, None, :]
        query_pos = first_row + jnp.arange(block_rows, dtype=jnp.int32)
        causal = key_pos[None, :] <= query_pos[:, None]
        scores = jnp.where(causal, scores, -jnp.inf)
        row_max = lax.optimization_barrier(jnp.max(scores, axis=-1, keepdims=True))
        weight = jnp.exp(scores - row_max)
        row_total = lax.optimization_barrier(jnp.sum(weight, axis=-1))
        weight_b = lax.optimization_barrier(weight.astype(jnp.bfloat16)).astype(jnp.float32)
        mixed_heads = jnp.einsum('grtn,ngd->grtd', weight_b, value_part) / row_total[..., None]
        mixed_heads = jnp.transpose(mixed_heads, (2, 0, 1, 3)).reshape(block_rows, ASKING_ATTENDERS * HEAD)
        return mixed_heads.astype(jnp.bfloat16)
    blocks = lax.map(one_block, jnp.arange(seq_len // block_rows, dtype=jnp.int32))
    return blocks.reshape(seq_len, ASKING_ATTENDERS * HEAD)

def reference(queries, keys_values, log_gate_cum, mix_weight, mix_gain, moe_in, moe_gain, routes, route_weight, expert_gate, expert_up, expert_down):
    attended = attend_reference(queries, keys_values, log_gate_cum)
    seq_len = attended.shape[0]
    head_width = ASKING_ATTENDERS * HEAD // N_TP
    projected = jnp.zeros((seq_len, D), jnp.float32)
    for shard_index in range(N_TP):
        head_part = jnp.dot(attended[:, shard_index * head_width:(shard_index + 1) * head_width], mix_weight[shard_index * head_width:(shard_index + 1) * head_width], preferred_element_type=jnp.float32).astype(jnp.bfloat16)
        projected = projected + lax.optimization_barrier(head_part).astype(jnp.float32)
    mix_result = rms_scale(projected, mix_gain).astype(jnp.bfloat16)
    normed = rms_scale(moe_in, moe_gain).astype(jnp.bfloat16)
    token_count = normed.shape[0]
    flat_routes = routes.reshape(-1).astype(jnp.int32)
    flat_weight = route_weight.reshape(-1)
    order = jnp.argsort(flat_routes, stable=True).astype(jnp.int32)
    most_rows = N_EP * N_TP * CAP
    expert_ids = jnp.arange(EXPERTS, dtype=jnp.int32)
    counts = lax.optimization_barrier(jnp.sum((flat_routes[:, None] == expert_ids[None, :]).astype(jnp.int32), axis=0))
    starts = (jnp.cumsum(counts) - counts).astype(jnp.int32)
    order_padded = jnp.concatenate([order, jnp.zeros((most_rows,), jnp.int32)])
    ff_width = FF // N_TP

    def one_expert(accum, inputs):
        gate_here, up_here, down_here, first_slot, count_here = inputs
        picked = lax.dynamic_slice_in_dim(order_padded, first_slot, most_rows, 0)
        valid = jnp.arange(most_rows, dtype=jnp.int32) < count_here
        token_ids = (picked // TOPK).astype(jnp.int32)
        rows_in = normed[token_ids]
        hidden = (jax.nn.silu(jnp.dot(rows_in, gate_here, preferred_element_type=jnp.float32)) * jnp.dot(rows_in, up_here, preferred_element_type=jnp.float32)).astype(jnp.bfloat16)
        summed = jnp.zeros((most_rows, D), jnp.float32)
        for shard_index in range(N_TP):
            width_part = jnp.dot(hidden[:, shard_index * ff_width:(shard_index + 1) * ff_width], down_here[shard_index * ff_width:(shard_index + 1) * ff_width], preferred_element_type=jnp.float32).astype(jnp.bfloat16)
            summed = summed + lax.optimization_barrier(width_part).astype(jnp.float32)
        expert_out = lax.optimization_barrier(summed.astype(jnp.bfloat16)).astype(jnp.float32)
        scaled = jnp.where(valid, flat_weight[picked], 0.0)
        accum = accum.at[token_ids].add(scaled[:, None] * expert_out)
        return (accum, None)
    accum, _ = lax.scan(one_expert, jnp.zeros((token_count, D), jnp.float32), (expert_gate, expert_up, expert_down, starts, counts))
    moe_result = accum.astype(jnp.bfloat16)
    return (mix_result, moe_result)
```

```python
import jax
import jax.numpy as jnp
from jax import lax
from jax.experimental import pallas as pl
from jax.experimental.pallas import tpu as pltpu
from jax.sharding import PartitionSpec as P


HEAD = 64
EPSILON = 1e-06
NEGATIVE = -1e30
LANES = 256
KEY_BLOCK = 1024
LOG2E = 1.4426950408889634


def slot_positions(routes, experts):
    tokens = routes.shape[1]
    first, second = routes[0:1, :], routes[1:2, :]
    expert_ids = lax.broadcasted_iota(jnp.int32, (experts, tokens), 0)
    one_first = (first == expert_ids).astype(jnp.float32)
    one_second = (second == expert_ids).astype(jnp.float32)
    row = lax.broadcasted_iota(jnp.int32, (tokens, tokens), 0)
    col = lax.broadcasted_iota(jnp.int32, (tokens, tokens), 1)
    earlier = (row < col).astype(jnp.float32).astype(jnp.bfloat16)
    count_first = jnp.dot(
        one_first.astype(jnp.bfloat16), earlier, preferred_element_type=jnp.float32
    )
    count_second = jnp.dot(
        one_second.astype(jnp.bfloat16), earlier, preferred_element_type=jnp.float32
    ) + jnp.sum(one_first, axis=1, keepdims=True)
    place_first = jnp.sum(one_first * count_first, axis=0, keepdims=True).astype(jnp.int32)
    place_second = jnp.sum(one_second * count_second, axis=0, keepdims=True).astype(jnp.int32)
    return (first, place_first), (second, place_second)


def slot_masks(expert, place, experts):
    tokens = expert.shape[1]
    eight = lax.broadcasted_iota(jnp.int32, (experts * 8, tokens), 0)
    ninth = lax.broadcasted_iota(jnp.int32, (experts, tokens), 0)
    in_eight = eight == jnp.where(place < 8, expert * 8 + place, -1)
    in_ninth = ninth == jnp.where(place == 8, expert, -1)
    return in_eight, in_ninth


def as_bf16(mask):
    return mask.astype(jnp.float32).astype(jnp.bfloat16)


def as_rows(block):
    wide = block.astype(jnp.float32)
    return wide.reshape(-1, block.shape[-1]).astype(jnp.bfloat16)


def dispatch_kernel(routes_ref, tokens_ref, out_ref, ninth_ref):
    experts = out_ref.shape[0]
    groups = tokens_ref.shape[1] // LANES
    picks = slot_positions(routes_ref[...], experts)
    (a8, a9), (b8, b9) = [slot_masks(e, p, experts) for e, p in picks]
    pick8 = as_bf16(jnp.logical_or(a8, b8))
    pick9 = as_bf16(jnp.logical_or(a9, b9))
    for g in range(groups):
        columns = tokens_ref[:, g * LANES : (g + 1) * LANES]
        chosen = jnp.dot(pick8, columns, preferred_element_type=jnp.float32)
        out_ref[:, g * 8 : (g + 1) * 8, :] = chosen.reshape(experts, 8, LANES).astype(jnp.bfloat16)
        last = jnp.dot(pick9, columns, preferred_element_type=jnp.float32)
        for half in range(LANES // 128):
            ninth_ref[half, pl.ds(g, experts, stride=groups), :] = last[
                :, half * 128 : (half + 1) * 128
            ]
    whole = jnp.concatenate([ninth_ref[half] for half in range(LANES // 128)], axis=1)
    out_ref[:, 8 * groups :, :] = whole.reshape(experts, groups, LANES).astype(jnp.bfloat16)


def hidden_kernel(
    received_ref, gain_ref,
    g0, u0, g1, u1, g2, u2, g3, u3,
    hidden_ref,
    gate_buf, up_buf, tokens_ref, ninth_ref, sems,
):
    sources = received_ref.shape[0]
    groups = received_ref.shape[1] // 9
    width = groups * LANES
    eights = sources * 8
    ff = g0.shape[1]
    copies = []
    for n, (g, u) in enumerate(((g0, u0), (g1, u1), (g2, u2), (g3, u3))):
        copies.append(pltpu.make_async_copy(g, gate_buf.at[n], sems.at[2 * n]))
        copies.append(pltpu.make_async_copy(u, up_buf.at[n], sems.at[2 * n + 1]))
    for c in copies:
        c.start()

    ninth = received_ref[:, 8 * groups :, :].astype(jnp.float32).reshape(sources * groups, LANES)
    for h in range(LANES // 128):
        ninth_ref[h] = ninth[:, h * 128 : (h + 1) * 128]

    def eight_rows(g):
        block = received_ref[:, g * 8 : (g + 1) * 8, :].astype(jnp.float32)
        return block.reshape(eights, LANES)

    def ninth_rows(g):
        return jnp.concatenate(
            [ninth_ref[h, pl.ds(g, sources, stride=groups), :] for h in range(LANES // 128)], axis=1
        )

    square8 = jnp.zeros((eights, LANES), jnp.float32)
    square9 = jnp.zeros((sources, LANES), jnp.float32)
    for g in range(groups):
        x = eight_rows(g)
        square8 = square8 + x * x
        y = ninth_rows(g)
        square9 = square9 + y * y
    scale8 = lax.rsqrt(jnp.sum(square8, axis=1, keepdims=True) / width + EPSILON)
    scale9 = lax.rsqrt(jnp.sum(square9, axis=1, keepdims=True) / width + EPSILON)
    for g in range(groups):
        gain = gain_ref[:, g * LANES : (g + 1) * LANES]
        tokens_ref[:eights, g * LANES : (g + 1) * LANES] = (
            eight_rows(g) * scale8 * gain
        ).astype(jnp.bfloat16)
        tokens_ref[eights:, g * LANES : (g + 1) * LANES] = (
            ninth_rows(g) * scale9 * gain
        ).astype(jnp.bfloat16)

    for n in range(4):
        copies[2 * n].wait()
        copies[2 * n + 1].wait()
        gated = jnp.dot(tokens_ref[...], gate_buf[n], preferred_element_type=jnp.float32)
        lifted = jnp.dot(tokens_ref[...], up_buf[n], preferred_element_type=jnp.float32)
        hidden_ref[:, n * ff : (n + 1) * ff] = (
            gated / (1.0 + jnp.exp(-gated)) * lifted
        ).astype(jnp.bfloat16)


def down_kernel(hidden_ref, d0, d1, d2, d3a, d3b, out_ref, down_buf, ninth_ref, sems):
    sources = out_ref.shape[0]
    groups = out_ref.shape[1] // 9
    eights = sources * 8
    ff = d0.shape[0]
    half = d3a.shape[0]
    pieces = ((d0, 0, ff), (d1, ff, ff), (d2, 2 * ff, ff), (d3a, 3 * ff, half), (d3b, 3 * ff + half, half))
    copies = []
    for g in range(groups):
        columns = pl.ds(g * LANES, LANES)
        copies.append(
            [
                pltpu.make_async_copy(
                    d.at[:, columns], down_buf.at[g, pl.ds(at, size), :], sems.at[5 * g + n]
                )
                for n, (d, at, size) in enumerate(pieces)
            ]
        )
    for group in copies:
        for c in group:
            c.start()
    for g in range(groups):
        for c in copies[g]:
            c.wait()
        result = jnp.dot(hidden_ref[...], down_buf[g], preferred_element_type=jnp.float32)
        out_ref[:, g * 8 : (g + 1) * 8, :] = (
            result[:eights].reshape(sources, 8, LANES).astype(jnp.bfloat16)
        )
        for h in range(LANES // 128):
            ninth_ref[h, pl.ds(g, sources, stride=groups), :] = result[
                eights:, h * 128 : (h + 1) * 128
            ]
    whole = jnp.concatenate([ninth_ref[h] for h in range(LANES // 128)], axis=1)
    out_ref[:, 8 * groups :, :] = whole.reshape(sources, groups, LANES).astype(jnp.bfloat16)


def attention_kernel(
    place_ref, queries_ref, keys_ref, gate_ref, mix_ref, after_ref,
    own_ref, right_ref, left_ref, far_ref,
    scaled_ref, sums_ref, top_ref, mixed_ref,
):
    rows = queries_ref.shape[0]
    heads = queries_ref.shape[1] // HEAD
    block = min(KEY_BLOCK, keys_ref.shape[0])
    quarter = own_ref.shape[0]
    first_row = place_ref[0] * rows
    for h in range(heads):
        part = queries_ref[:, h * HEAD : (h + 1) * HEAD].astype(jnp.float32) * HEAD ** (-0.5)
        scaled_ref[h] = jnp.concatenate([part, jnp.zeros_like(part)], axis=1).astype(jnp.bfloat16)
    sums_ref[...] = jnp.zeros_like(sums_ref)
    top_ref[...] = jnp.full_like(top_ref, NEGATIVE)
    value_lane = lax.broadcasted_iota(jnp.int32, (block, 2 * HEAD), 1) >= HEAD

    def fold(start, masked):
        pairs = keys_ref[pl.ds(start, block), :]
        values = jnp.where(value_lane, pairs.astype(jnp.float32), 1.0).astype(jnp.bfloat16)
        if masked:
            query_pos = first_row + lax.broadcasted_iota(jnp.int32, (rows, block), 0)
            key_pos = start + lax.broadcasted_iota(jnp.int32, (rows, block), 1)
            causal = key_pos <= query_pos
        scores = [
            lax.dot_general(
                scaled_ref[h], pairs, (((1,), (1,)), ((), ())), preferred_element_type=jnp.float32
            )
            * LOG2E
            - gate_ref[h : h + 1, pl.ds(start, block)] * LOG2E
            for h in range(heads)
        ]
        folded = []
        for h in range(heads):
            score = scores[h]
            if masked:
                score = jnp.where(causal, score, NEGATIVE)
            old_top = top_ref[h][:, 0:1]
            new_top = jnp.maximum(old_top, jnp.max(score, axis=1, keepdims=True))
            weight = jnp.exp2(score - new_top)
            if masked:
                weight = jnp.where(causal, weight, 0.0)
            top_ref[h] = jnp.broadcast_to(new_top, top_ref.shape[1:])
            folded.append((weight.astype(jnp.bfloat16), jnp.exp2(old_top - new_top)))
        for h in range(heads):
            weight, kept = folded[h]
            sums_ref[h] = sums_ref[h] * kept + jnp.dot(
                weight, values, preferred_element_type=jnp.float32
            )

    whole_blocks = first_row // block

    def step(i, carry):
        fold(pl.multiple_of(i * block, block), False)
        return carry

    lax.fori_loop(0, whole_blocks, step, 0)
    fold(pl.multiple_of(whole_blocks * block, block), True)
    mixed = []
    for h in range(heads):
        total = sums_ref[h]
        mixed.append(total[:, HEAD:] / total[:, 0:1])
    mixed_ref[...] = jnp.concatenate(mixed, axis=1).astype(jnp.bfloat16)
    parts = 4
    for shift, out_ref in ((0, own_ref), (1, right_ref), (3, left_ref), (2, far_ref)):
        at = pl.multiple_of(((place_ref[1] + shift) % parts) * quarter, quarter)
        out_ref[...] = jnp.dot(
            mixed_ref[pl.ds(at, quarter), :], mix_ref[...], preferred_element_type=jnp.float32
        ).astype(jnp.bfloat16)


def combine_kernel(routes_ref, weight_ref, returned_ref, out_ref, ninth_ref):
    experts = returned_ref.shape[0]
    groups = returned_ref.shape[1] // 9
    tokens = routes_ref.shape[1]
    picks = slot_positions(routes_ref[...], experts)
    masks = [[as_bf16(m) for m in slot_masks(e, p, experts)] for e, p in picks]
    row = lax.broadcasted_iota(jnp.int32, (tokens, tokens), 0)
    col = lax.broadcasted_iota(jnp.int32, (tokens, tokens), 1)
    weights = [
        jnp.sum(jnp.where(row == col, weight_ref[k : k + 1, :], 0.0), axis=1, keepdims=True)
        for k in range(2)
    ]
    ninth = returned_ref[:, 8 * groups :, :].astype(jnp.float32).reshape(experts * groups, LANES)
    for h in range(LANES // 128):
        ninth_ref[h] = ninth[:, h * 128 : (h + 1) * 128]
    over_slots = (((0,), (0,)), ((), ()))
    for g in range(groups):
        eight = as_rows(returned_ref[:, g * 8 : (g + 1) * 8, :])
        last = jnp.concatenate(
            [ninth_ref[h, pl.ds(g, experts, stride=groups), :] for h in range(LANES // 128)], axis=1
        ).astype(jnp.bfloat16)
        total = 0.0
        for k in range(2):
            chosen = lax.dot_general(
                masks[k][0], eight, over_slots, preferred_element_type=jnp.float32
            ) + lax.dot_general(masks[k][1], last, over_slots, preferred_element_type=jnp.float32)
            total = total + weights[k] * chosen
        out_ref[:, g * LANES : (g + 1) * LANES] = total.astype(jnp.bfloat16)


def rms_scale(values, gain):
    return values * lax.rsqrt(jnp.mean(values * values, axis=-1, keepdims=True) + EPSILON) * gain


VMEM = pl.BlockSpec(memory_space=pltpu.VMEM)
SMEM = pl.BlockSpec(memory_space=pltpu.SMEM)
ANY = pl.BlockSpec(memory_space=pl.ANY)


def body(
    queries,
    keys_values,
    log_gate_cum,
    mix_weight,
    mix_gain,
    moe_in,
    moe_gain,
    routes,
    route_weight,
    expert_gate,
    expert_up,
    expert_down,
):
    ep_count = lax.axis_size("ep")
    tp_count = lax.axis_size("tp")
    place = jnp.stack([lax.axis_index("ep"), lax.axis_index("tp")]).astype(jnp.int32)
    to_right = [(i, (i + 1) % tp_count) for i in range(tp_count)]
    to_left = [(i, (i - 1) % tp_count) for i in range(tp_count)]
    to_far = [(i, (i + 2) % tp_count) for i in range(tp_count)]
    rows_here, width = moe_in.shape
    groups = width // LANES
    slot_rows = ep_count * 9
    ff = expert_gate.shape[2]
    lane_routes, lane_weight = routes.T, route_weight.T

    gate, up, down = expert_gate[0], expert_up[0], expert_down[0]
    gate_r = lax.ppermute(gate, "tp", to_right)
    up_l = lax.ppermute(up, "tp", to_left)
    up_r = lax.ppermute(up, "tp", to_right)
    gate_l = lax.ppermute(gate, "tp", to_left)
    gate_f = lax.ppermute(gate_r, "tp", to_right)
    up_f = lax.ppermute(up_l, "tp", to_left)
    down_r = lax.ppermute(down, "tp", to_right)
    down_l = lax.ppermute(down, "tp", to_left)
    down_fa = lax.ppermute(down_r[: ff // 2], "tp", to_right)
    down_fb = lax.ppermute(down_l[ff // 2 :], "tp", to_left)

    all_pairs = lax.all_gather(keys_values, "ep", axis=0, tiled=True)

    exchange_shape = jax.ShapeDtypeStruct((ep_count, 9 * groups, LANES), jnp.bfloat16)
    outgoing = pl.pallas_call(
        dispatch_kernel,
        out_shape=exchange_shape,
        in_specs=[VMEM, VMEM],
        out_specs=VMEM,
        scratch_shapes=[pltpu.VMEM((LANES // 128, ep_count * groups, 128), jnp.float32)],
        name="dispatch_rows",
    )(lane_routes, moe_in)
    received = lax.all_to_all(outgoing, "ep", 0, 0, tiled=True)
    hidden = pl.pallas_call(
        hidden_kernel,
        out_shape=jax.ShapeDtypeStruct((slot_rows, tp_count * ff), jnp.bfloat16),
        in_specs=[VMEM, VMEM] + [ANY] * 8,
        out_specs=VMEM,
        scratch_shapes=[
            pltpu.VMEM((tp_count, width, ff), jnp.bfloat16),
            pltpu.VMEM((tp_count, width, ff), jnp.bfloat16),
            pltpu.VMEM((slot_rows, width), jnp.bfloat16),
            pltpu.VMEM((LANES // 128, ep_count * groups, 128), jnp.float32),
            pltpu.SemaphoreType.DMA((8,)),
        ],
        cost_estimate=pl.CostEstimate(
            flops=4 * slot_rows * width * ff * tp_count,
            bytes_accessed=12_000_000,
            transcendentals=0,
        ),
        name="hidden_rows",
    )(
        received, moe_gain.reshape(1, width),
        gate, up, gate_r, up_r, gate_l, up_l, gate_f, up_f,
    )
    results = pl.pallas_call(
        down_kernel,
        out_shape=exchange_shape,
        in_specs=[VMEM] + [ANY] * 5,
        out_specs=VMEM,
        scratch_shapes=[
            pltpu.VMEM((groups, tp_count * ff, LANES), jnp.bfloat16),
            pltpu.VMEM((LANES // 128, ep_count * groups, 128), jnp.float32),
            pltpu.SemaphoreType.DMA((5 * groups,)),
        ],
        cost_estimate=pl.CostEstimate(
            flops=2 * slot_rows * width * ff * tp_count,
            bytes_accessed=8_000_000,
            transcendentals=0,
        ),
        name="down_rows",
    )(hidden, down, down_r, down_l, down_fa, down_fb)
    returned = lax.all_to_all(results, "ep", 0, 0, tiled=True)
    rows, head_width = queries.shape
    heads = head_width // HEAD
    quarter = rows // tp_count
    quarter_shape = jax.ShapeDtypeStruct((quarter, width), jnp.bfloat16)
    own, right, left, far = pl.pallas_call(
        attention_kernel,
        out_shape=[quarter_shape] * 4,
        in_specs=[SMEM, VMEM, VMEM, VMEM, VMEM, ANY],
        out_specs=[VMEM] * 4,
        scratch_shapes=[
            pltpu.VMEM((heads, rows, 2 * HEAD), jnp.bfloat16),
            pltpu.VMEM((heads, rows, 2 * HEAD), jnp.float32),
            pltpu.VMEM((heads, rows, 128), jnp.float32),
            pltpu.VMEM((rows, head_width), jnp.bfloat16),
        ],
        cost_estimate=pl.CostEstimate(
            flops=30_000_000_000, bytes_accessed=5_000_000, transcendentals=0
        ),
        name="attend_rows",
    )(place, queries, all_pairs, log_gate_cum, mix_weight, results)
    from_left = lax.ppermute(right, "tp", to_right)
    from_right = lax.ppermute(left, "tp", to_left)
    from_far = lax.ppermute(far, "tp", to_far)
    projected = (
        own.astype(jnp.float32)
        + from_left.astype(jnp.float32)
        + from_right.astype(jnp.float32)
        + from_far.astype(jnp.float32)
    )
    mix_result = rms_scale(projected, mix_gain).astype(jnp.bfloat16)
    moe_result = pl.pallas_call(
        combine_kernel,
        out_shape=jax.ShapeDtypeStruct((rows_here, width), jnp.bfloat16),
        in_specs=[VMEM, VMEM, VMEM],
        out_specs=VMEM,
        scratch_shapes=[pltpu.VMEM((LANES // 128, ep_count * groups, 128), jnp.float32)],
        name="combine_rows",
    )(lane_routes, lane_weight, returned)
    return (mix_result, moe_result)


def solution(mesh):
    in_specs = (
        P("ep", "tp"),
        P("ep", "tp"),
        P("tp", None),
        P("tp", None),
        P(),
        P(("ep", "tp"), None),
        P(),
        P(("ep", "tp"), None),
        P(("ep", "tp"), None),
        P("ep", None, "tp"),
        P("ep", None, "tp"),
        P("ep", "tp", None),
    )
    out_specs = (P(("ep", "tp"), None), P(("ep", "tp"), None))
    return jax.shard_map(body, mesh=mesh, in_specs=in_specs, out_specs=out_specs, check_vma=False)
```

```python
import jax
import jax.numpy as jnp
from jax import lax
from jax.experimental import pallas as pl
from jax.experimental.pallas import tpu as pltpu
from jax.sharding import PartitionSpec as P


HEAD = 64
EPSILON = 1e-06
NEGATIVE = -1e30
LANES = 256
LOG2E = 1.4426950408889634


def slot_positions(routes, experts):
    tokens = routes.shape[1]
    first, second = routes[0:1, :], routes[1:2, :]
    expert_ids = lax.broadcasted_iota(jnp.int32, (experts, tokens), 0)
    one_first = (first == expert_ids).astype(jnp.float32)
    one_second = (second == expert_ids).astype(jnp.float32)
    row = lax.broadcasted_iota(jnp.int32, (tokens, tokens), 0)
    col = lax.broadcasted_iota(jnp.int32, (tokens, tokens), 1)
    earlier = (row < col).astype(jnp.float32).astype(jnp.bfloat16)
    count_first = jnp.dot(
        one_first.astype(jnp.bfloat16), earlier, preferred_element_type=jnp.float32
    )
    count_second = jnp.dot(
        one_second.astype(jnp.bfloat16), earlier, preferred_element_type=jnp.float32
    ) + jnp.sum(one_first, axis=1, keepdims=True)
    place_first = jnp.sum(one_first * count_first, axis=0, keepdims=True).astype(jnp.int32)
    place_second = jnp.sum(one_second * count_second, axis=0, keepdims=True).astype(jnp.int32)
    return (first, place_first), (second, place_second)


def slot_masks(expert, place, experts):
    tokens = expert.shape[1]
    eight = lax.broadcasted_iota(jnp.int32, (experts * 8, tokens), 0)
    ninth = lax.broadcasted_iota(jnp.int32, (experts, tokens), 0)
    in_eight = eight == jnp.where(place < 8, expert * 8 + place, -1)
    in_ninth = ninth == jnp.where(place == 8, expert, -1)
    return in_eight, in_ninth


def as_bf16(mask):
    return mask.astype(jnp.float32).astype(jnp.bfloat16)


def as_rows(block):
    wide = block.astype(jnp.float32)
    return wide.reshape(-1, block.shape[-1]).astype(jnp.bfloat16)


def dispatch_kernel(routes_ref, tokens_ref, out_ref, ninth_ref):
    experts = out_ref.shape[0]
    groups = tokens_ref.shape[1] // LANES
    picks = slot_positions(routes_ref[...], experts)
    (a8, a9), (b8, b9) = [slot_masks(e, p, experts) for e, p in picks]
    pick8 = as_bf16(jnp.logical_or(a8, b8))
    pick9 = as_bf16(jnp.logical_or(a9, b9))
    for g in range(groups):
        columns = tokens_ref[:, g * LANES : (g + 1) * LANES]
        chosen = jnp.dot(pick8, columns, preferred_element_type=jnp.float32)
        out_ref[:, g * 8 : (g + 1) * 8, :] = chosen.reshape(experts, 8, LANES).astype(jnp.bfloat16)
        last = jnp.dot(pick9, columns, preferred_element_type=jnp.float32)
        for half in range(LANES // 128):
            ninth_ref[half, pl.ds(g, experts, stride=groups), :] = last[
                :, half * 128 : (half + 1) * 128
            ]
    whole = jnp.concatenate([ninth_ref[half] for half in range(LANES // 128)], axis=1)
    out_ref[:, 8 * groups :, :] = whole.reshape(experts, groups, LANES).astype(jnp.bfloat16)


def silu_product(tokens, gate, up):
    gated = jnp.dot(tokens, gate, preferred_element_type=jnp.float32)
    lifted = jnp.dot(tokens, up, preferred_element_type=jnp.float32)
    return (gated / (1.0 + jnp.exp(-gated)) * lifted).astype(jnp.bfloat16)


def near_kernel(
    received_ref, gain_ref, g0, u0, g1, u1, g2, u2,
    hidden_ref, tokens_ref,
    ninth_ref,
):
    sources = received_ref.shape[0]
    groups = received_ref.shape[1] // 9
    width = groups * LANES
    eights = sources * 8
    ff = g0.shape[1]
    ninth = received_ref[:, 8 * groups :, :].astype(jnp.float32).reshape(sources * groups, LANES)
    for h in range(LANES // 128):
        ninth_ref[h] = ninth[:, h * 128 : (h + 1) * 128]

    def eight_rows(g):
        block = received_ref[:, g * 8 : (g + 1) * 8, :].astype(jnp.float32)
        return block.reshape(eights, LANES)

    def ninth_rows(g):
        return jnp.concatenate(
            [ninth_ref[h, pl.ds(g, sources, stride=groups), :] for h in range(LANES // 128)], axis=1
        )

    square8 = jnp.zeros((eights, LANES), jnp.float32)
    square9 = jnp.zeros((sources, LANES), jnp.float32)
    for g in range(groups):
        x = eight_rows(g)
        square8 = square8 + x * x
        y = ninth_rows(g)
        square9 = square9 + y * y
    scale8 = lax.rsqrt(jnp.sum(square8, axis=1, keepdims=True) / width + EPSILON)
    scale9 = lax.rsqrt(jnp.sum(square9, axis=1, keepdims=True) / width + EPSILON)
    for g in range(groups):
        gain = gain_ref[:, g * LANES : (g + 1) * LANES]
        tokens_ref[:eights, g * LANES : (g + 1) * LANES] = (
            eight_rows(g) * scale8 * gain
        ).astype(jnp.bfloat16)
        tokens_ref[eights:, g * LANES : (g + 1) * LANES] = (
            ninth_rows(g) * scale9 * gain
        ).astype(jnp.bfloat16)
    for n, (gate, up) in enumerate(((g0, u0), (g1, u1), (g2, u2))):
        hidden_ref[:, n * ff : (n + 1) * ff] = silu_product(tokens_ref[...], gate[...], up[...])


def far_kernel(tokens_ref, gate, up, near_ref, d0, d1, d2, hidden_ref, sum_ref):
    hidden_ref[...] = silu_product(tokens_ref[...], gate[...], up[...])
    for g in range(d0.shape[1] // LANES):
        columns = slice(g * LANES, (g + 1) * LANES)
        down = jnp.concatenate([d[:, columns] for d in (d0, d1, d2)], axis=0)
        sum_ref[:, columns] = jnp.dot(near_ref[...], down, preferred_element_type=jnp.float32)


def down_kernel(sum_ref, far_ref, d3a, d3b, out_ref, built_ref, ninth_ref, sems):
    sources = out_ref.shape[0]
    groups = out_ref.shape[1] // 9
    eights = sources * 8
    leaving = []

    def leave(part, size):
        rows = pl.ds(part * 8, size)
        copy = pltpu.make_async_copy(
            built_ref.at[:, rows, :], out_ref.at[:, rows, :], sems.at[part]
        )
        copy.start()
        leaving.append(copy)

    for g in range(groups):
        columns = slice(g * LANES, (g + 1) * LANES)
        result = sum_ref[:, columns] + jnp.dot(
            far_ref[...],
            jnp.concatenate([d3a[:, columns], d3b[:, columns]], axis=0),
            preferred_element_type=jnp.float32,
        )
        built_ref[:, g * 8 : (g + 1) * 8, :] = (
            result[:eights].reshape(sources, 8, LANES).astype(jnp.bfloat16)
        )
        leave(g, 8)
        for h in range(LANES // 128):
            ninth_ref[h, pl.ds(g, sources, stride=groups), :] = result[
                eights:, h * 128 : (h + 1) * 128
            ]
    whole = jnp.concatenate([ninth_ref[h] for h in range(LANES // 128)], axis=1)
    built_ref[:, 8 * groups :, :] = whole.reshape(sources, groups, LANES).astype(jnp.bfloat16)
    leave(groups, groups)
    for copy in leaving:
        copy.wait()


def stack_kernel(*refs):
    rows = refs[0].shape[0]
    for n, ref in enumerate(refs[:-1]):
        refs[-1][n * rows : (n + 1) * rows, :] = ref[...]


def attention_kernel(
    place_ref, queries_ref, gate_ref, mix_ref,
    k0, k1, k2, k3, k4, k5, k6, k7,
    own_ref, right_ref, left_ref, far_ref,
    scaled_ref, sums_ref, top_ref, mixed_ref,
):
    rows = queries_ref.shape[0]
    heads = queries_ref.shape[1] // HEAD
    quarter = own_ref.shape[0]
    plane, column, core = place_ref[0], place_ref[1], place_ref[2]
    sources = ((k0, 0, 0), (k1, 1, 0), (k2, 3, 0), (k3, 2, 0), (k4, 0, 1), (k5, 1, 1), (k6, 3, 1), (k7, 2, 1))
    for h in range(heads):
        part = queries_ref[:, h * HEAD : (h + 1) * HEAD].astype(jnp.float32) * HEAD ** (-0.5)
        scaled_ref[h] = jnp.concatenate([part, jnp.zeros_like(part)], axis=1).astype(jnp.bfloat16)
    sums_ref[...] = jnp.zeros_like(sums_ref)
    top_ref[...] = jnp.full_like(top_ref, NEGATIVE)
    own_index = plane * 8 + column * 2 + core

    def fold(pairs, gates, causal):
        lane = lax.broadcasted_iota(jnp.int32, pairs.shape, 1)
        values = jnp.where(lane >= HEAD, pairs.astype(jnp.float32), 1.0).astype(jnp.bfloat16)
        scores = [
            lax.dot_general(
                scaled_ref[h], pairs, (((1,), (1,)), ((), ())), preferred_element_type=jnp.float32
            )
            * LOG2E
            - gates[h : h + 1, :] * LOG2E
            for h in range(heads)
        ]
        folded = []
        for h in range(heads):
            score = scores[h]
            if causal is not None:
                score = jnp.where(causal, score, NEGATIVE)
            old_top = top_ref[h][:, 0:1]
            new_top = jnp.maximum(old_top, jnp.max(score, axis=1, keepdims=True))
            weight = jnp.exp2(score - new_top)
            top_ref[h] = jnp.broadcast_to(new_top, top_ref.shape[1:])
            folded.append((weight.astype(jnp.bfloat16), jnp.exp2(old_top - new_top)))
        for h in range(heads):
            weight, kept = folded[h]
            sums_ref[h] = sums_ref[h] * kept + jnp.dot(
                weight, values, preferred_element_type=jnp.float32
            )

    fold(
        k0[:rows, :],
        gate_ref[:, pl.ds(pl.multiple_of(own_index * rows, rows), rows)],
        lax.broadcasted_iota(jnp.int32, (rows, rows), 1)
        <= lax.broadcasted_iota(jnp.int32, (rows, rows), 0),
    )

    def step(back, carry):
        at = pl.multiple_of(back * rows, rows)
        for group in range(2):
            pairs, gates = [], []
            for keys, across, other in sources[group * 4 : (group + 1) * 4]:
                index = (plane - back) * 8 + ((column + 4 - across) % 4) * 2 + (core + other) % 2
                gate = gate_ref[:, pl.ds(pl.multiple_of(index * rows, rows), rows)]
                pairs.append(keys[pl.ds(at, rows), :])
                gates.append(jnp.where(index < own_index, gate, -NEGATIVE))
            fold(jnp.concatenate(pairs, axis=0), jnp.concatenate(gates, axis=1), None)
        return carry

    lax.fori_loop(0, plane + 1, step, 0)
    mixed = []
    for h in range(heads):
        total = sums_ref[h]
        mixed.append(total[:, HEAD:] / total[:, 0:1])
    mixed_ref[...] = jnp.concatenate(mixed, axis=1).astype(jnp.bfloat16)
    parts = 4
    for shift, out_ref in ((0, own_ref), (1, right_ref), (3, left_ref), (2, far_ref)):
        at = pl.multiple_of(((place_ref[3] + shift) % parts) * quarter, quarter)
        out_ref[...] = jnp.dot(
            mixed_ref[pl.ds(at, quarter), :], mix_ref[...], preferred_element_type=jnp.float32
        ).astype(jnp.bfloat16)


def combine_kernel(routes_ref, weight_ref, returned_ref, out_ref, ninth_ref):
    experts = returned_ref.shape[0]
    groups = returned_ref.shape[1] // 9
    tokens = routes_ref.shape[1]
    picks = slot_positions(routes_ref[...], experts)
    masks = [[as_bf16(m) for m in slot_masks(e, p, experts)] for e, p in picks]
    row = lax.broadcasted_iota(jnp.int32, (tokens, tokens), 0)
    col = lax.broadcasted_iota(jnp.int32, (tokens, tokens), 1)
    weights = [
        jnp.sum(jnp.where(row == col, weight_ref[k : k + 1, :], 0.0), axis=1, keepdims=True)
        for k in range(2)
    ]
    ninth = returned_ref[:, 8 * groups :, :].astype(jnp.float32).reshape(experts * groups, LANES)
    for h in range(LANES // 128):
        ninth_ref[h] = ninth[:, h * 128 : (h + 1) * 128]
    over_slots = (((0,), (0,)), ((), ()))
    for g in range(groups):
        eight = as_rows(returned_ref[:, g * 8 : (g + 1) * 8, :])
        last = jnp.concatenate(
            [ninth_ref[h, pl.ds(g, experts, stride=groups), :] for h in range(LANES // 128)], axis=1
        ).astype(jnp.bfloat16)
        total = 0.0
        for k in range(2):
            chosen = lax.dot_general(
                masks[k][0], eight, over_slots, preferred_element_type=jnp.float32
            ) + lax.dot_general(masks[k][1], last, over_slots, preferred_element_type=jnp.float32)
            total = total + weights[k] * chosen
        out_ref[:, g * LANES : (g + 1) * LANES] = total.astype(jnp.bfloat16)


def rms_scale(values, gain):
    return values * lax.rsqrt(jnp.mean(values * values, axis=-1, keepdims=True) + EPSILON) * gain


VMEM = pl.BlockSpec(memory_space=pltpu.VMEM)
SMEM = pl.BlockSpec(memory_space=pltpu.SMEM)
HBM = pl.BlockSpec(memory_space=pltpu.HBM)


def on_chip(array):
    return pltpu.with_memory_space_constraint(array, pltpu.VMEM)


def kept_on_chip(shape):
    return jax.ShapeDtypeStruct(shape, jnp.bfloat16)


def shift_pairs(down, across, other):
    return [
        (z * 8 + x * 2 + c, (z + down) % 8 * 8 + (x + across) % 4 * 2 + (c + other) % 2)
        for z in range(8)
        for x in range(4)
        for c in range(2)
    ]


def body(
    queries,
    keys_values,
    log_gate_cum,
    mix_weight,
    mix_gain,
    moe_in,
    moe_gain,
    routes,
    route_weight,
    expert_gate,
    expert_up,
    expert_down,
):
    ep_count = lax.axis_size("ep")
    tp_count = lax.axis_size("tp")
    ep_index = lax.axis_index("ep")
    place = jnp.stack(
        [ep_index // 8, ep_index // 2 % 4, ep_index % 2, lax.axis_index("tp")]
    ).astype(jnp.int32)
    to_right = [(i, (i + 1) % tp_count) for i in range(tp_count)]
    to_left = [(i, (i - 1) % tp_count) for i in range(tp_count)]
    to_far = [(i, (i + 2) % tp_count) for i in range(tp_count)]
    rows_here, width = moe_in.shape
    groups = width // LANES
    slot_rows = ep_count * 9
    ff = expert_gate.shape[2]
    lane_routes, lane_weight = routes.T, route_weight.T

    gate, up, down = expert_gate[0], expert_up[0], expert_down[0]
    gate_r = lax.ppermute(gate, "tp", to_right)
    up_l = lax.ppermute(up, "tp", to_left)
    up_r = lax.ppermute(up, "tp", to_right)
    gate_l = lax.ppermute(gate, "tp", to_left)
    down_r = lax.ppermute(down, "tp", to_right)
    down_l = lax.ppermute(down, "tp", to_left)
    gate_f = lax.ppermute(gate_r, "tp", to_right)
    up_f = lax.ppermute(up_l, "tp", to_left)
    down_fa = lax.ppermute(down_r[: ff // 2], "tp", to_right)
    down_fb = lax.ppermute(down_l[ff // 2 :], "tp", to_left)

    over_planes = [keys_values] + [
        lax.ppermute(keys_values, "ep", shift_pairs(d, 0, 0)) for d in range(1, 8)
    ]
    column_keys = pl.pallas_call(
        stack_kernel,
        out_shape=jax.ShapeDtypeStruct(
            (8 * keys_values.shape[0], keys_values.shape[1]), jnp.bfloat16
        ),
        in_specs=[VMEM] * 8,
        out_specs=VMEM,
        compiler_params=pltpu.CompilerParams(vmem_limit_bytes=8 * 2**20),
        name="stack_rows",
    )(*over_planes)
    core_keys = [column_keys] + [
        lax.ppermute(column_keys, "ep", shift_pairs(0, d, 0)) for d in (1, 3, 2)
    ]
    other_keys = [
        lax.ppermute(k, "ep", shift_pairs(0, 0, 1)) for k in core_keys
    ]

    exchange_shape = kept_on_chip((ep_count, 9 * groups, LANES))
    outgoing = pl.pallas_call(
        dispatch_kernel,
        out_shape=exchange_shape,
        in_specs=[VMEM, VMEM],
        out_specs=VMEM,
        scratch_shapes=[pltpu.VMEM((LANES // 128, ep_count * groups, 128), jnp.float32)],
        compiler_params=pltpu.CompilerParams(vmem_limit_bytes=16 * 2**20),
        name="dispatch_rows",
    )(lane_routes, moe_in)
    received = lax.all_to_all(outgoing, "ep", 0, 0, tiled=True)
    near, normed = pl.pallas_call(
        near_kernel,
        out_shape=[
            kept_on_chip((slot_rows, 3 * ff)),
            kept_on_chip((slot_rows, width)),
        ],
        in_specs=[VMEM] * 8,
        out_specs=[VMEM] * 2,
        scratch_shapes=[
            pltpu.VMEM((LANES // 128, ep_count * groups, 128), jnp.float32),
        ],
        cost_estimate=pl.CostEstimate(
            flops=12 * slot_rows * width * ff, bytes_accessed=9_000_000, transcendentals=0
        ),
        compiler_params=pltpu.CompilerParams(vmem_limit_bytes=24 * 2**20),
        name="near_rows",
    )(
        on_chip(received), moe_gain.reshape(1, width),
        gate, up, *[on_chip(w) for w in (gate_r, up_r, gate_l, up_l)],
    )
    far_hidden, near_sum = pl.pallas_call(
        far_kernel,
        out_shape=[
            kept_on_chip((slot_rows, ff)),
            jax.ShapeDtypeStruct((slot_rows, width), jnp.float32),
        ],
        in_specs=[VMEM] * 7,
        out_specs=[VMEM] * 2,
        cost_estimate=pl.CostEstimate(
            flops=10 * slot_rows * width * ff, bytes_accessed=9_000_000, transcendentals=0
        ),
        compiler_params=pltpu.CompilerParams(vmem_limit_bytes=16 * 2**20),
        name="far_rows",
    )(*[on_chip(v) for v in (normed, gate_f, up_f, near, down, down_r, down_l)])
    results = pl.pallas_call(
        down_kernel,
        out_shape=exchange_shape,
        in_specs=[VMEM] * 4,
        out_specs=HBM,
        scratch_shapes=[
            pltpu.VMEM((ep_count, 9 * groups, LANES), jnp.bfloat16),
            pltpu.VMEM((LANES // 128, ep_count * groups, 128), jnp.float32),
            pltpu.SemaphoreType.DMA((groups + 1,)),
        ],
        cost_estimate=pl.CostEstimate(
            flops=2 * slot_rows * width * ff,
            bytes_accessed=8_000_000,
            transcendentals=0,
        ),
        compiler_params=pltpu.CompilerParams(vmem_limit_bytes=56 * 2**20),
        name="down_rows",
    )(
        *[
            on_chip(v)
            for v in (near_sum, far_hidden, down_fa, down_fb)
        ]
    )
    returned = lax.all_to_all(results, "ep", 0, 0, tiled=True)
    rows, head_width = queries.shape
    heads = head_width // HEAD
    quarter = rows // tp_count
    quarter_shape = jax.ShapeDtypeStruct((quarter, width), jnp.bfloat16)
    own, right, left, far = pl.pallas_call(
        attention_kernel,
        out_shape=[quarter_shape] * 4,
        in_specs=[SMEM] + [VMEM] * 11,
        out_specs=[VMEM] * 4,
        scratch_shapes=[
            pltpu.VMEM((heads, rows, 2 * HEAD), jnp.bfloat16),
            pltpu.VMEM((heads, rows, 2 * HEAD), jnp.float32),
            pltpu.VMEM((heads, rows, 128), jnp.float32),
            pltpu.VMEM((rows, head_width), jnp.bfloat16),
        ],
        cost_estimate=pl.CostEstimate(
            flops=30_000_000_000, bytes_accessed=5_000_000, transcendentals=0
        ),
        compiler_params=pltpu.CompilerParams(vmem_limit_bytes=28 * 2**20),
        name="attend_rows",
    )(place, queries, log_gate_cum, mix_weight, *[on_chip(k) for k in core_keys + other_keys])
    from_left = lax.ppermute(right, "tp", to_right)
    from_right = lax.ppermute(left, "tp", to_left)
    from_far = lax.ppermute(far, "tp", to_far)
    projected = (
        own.astype(jnp.float32)
        + from_left.astype(jnp.float32)
        + from_right.astype(jnp.float32)
        + from_far.astype(jnp.float32)
    )
    mix_result = rms_scale(projected, mix_gain).astype(jnp.bfloat16)
    moe_result = pl.pallas_call(
        combine_kernel,
        out_shape=jax.ShapeDtypeStruct((rows_here, width), jnp.bfloat16),
        in_specs=[VMEM, VMEM, VMEM],
        out_specs=VMEM,
        scratch_shapes=[pltpu.VMEM((LANES // 128, ep_count * groups, 128), jnp.float32)],
        compiler_params=pltpu.CompilerParams(vmem_limit_bytes=16 * 2**20),
        name="combine_rows",
    )(lane_routes, lane_weight, on_chip(returned))
    return (mix_result, moe_result)


def solution(mesh):
    in_specs = (
        P("ep", "tp"),
        P("ep", "tp"),
        P("tp", None),
        P("tp", None),
        P(),
        P(("ep", "tp"), None),
        P(),
        P(("ep", "tp"), None),
        P(("ep", "tp"), None),
        P("ep", None, "tp"),
        P("ep", None, "tp"),
        P("ep", "tp", None),
    )
    out_specs = (P(("ep", "tp"), None), P(("ep", "tp"), None))
    return jax.shard_map(body, mesh=mesh, in_specs=in_specs, out_specs=out_specs, check_vma=False)
```

```python
import jax
import jax.numpy as jnp
from jax import lax
from jax.experimental import pallas as pl
from jax.experimental.pallas import tpu as pltpu
from jax.sharding import PartitionSpec as P


HEAD = 64
EPSILON = 1e-06
NEGATIVE = -1e30
LANES = 256
LOG2E = 1.4426950408889634


def slot_positions(routes, experts):
    tokens = routes.shape[1]
    first, second = routes[0:1, :], routes[1:2, :]
    expert_ids = lax.broadcasted_iota(jnp.int32, (experts, tokens), 0)
    one_first = (first == expert_ids).astype(jnp.float32)
    one_second = (second == expert_ids).astype(jnp.float32)
    row = lax.broadcasted_iota(jnp.int32, (tokens, tokens), 0)
    col = lax.broadcasted_iota(jnp.int32, (tokens, tokens), 1)
    earlier = (row < col).astype(jnp.float32).astype(jnp.bfloat16)
    count_first = jnp.dot(
        one_first.astype(jnp.bfloat16), earlier, preferred_element_type=jnp.float32
    )
    count_second = jnp.dot(
        one_second.astype(jnp.bfloat16), earlier, preferred_element_type=jnp.float32
    ) + jnp.sum(one_first, axis=1, keepdims=True)
    place_first = jnp.sum(one_first * count_first, axis=0, keepdims=True).astype(jnp.int32)
    place_second = jnp.sum(one_second * count_second, axis=0, keepdims=True).astype(jnp.int32)
    return (first, place_first), (second, place_second)


def slot_masks(expert, place, experts):
    tokens = expert.shape[1]
    eight = lax.broadcasted_iota(jnp.int32, (experts * 8, tokens), 0)
    ninth = lax.broadcasted_iota(jnp.int32, (experts, tokens), 0)
    in_eight = eight == jnp.where(place < 8, expert * 8 + place, -1)
    in_ninth = ninth == jnp.where(place == 8, expert, -1)
    return in_eight, in_ninth


def as_bf16(mask):
    return mask.astype(jnp.float32).astype(jnp.bfloat16)


def as_rows(block):
    wide = block.astype(jnp.float32)
    return wide.reshape(-1, block.shape[-1]).astype(jnp.bfloat16)


def dispatch_kernel(routes_ref, tokens_ref, out_ref, ninth_ref):
    experts = out_ref.shape[0]
    groups = tokens_ref.shape[1] // LANES
    picks = slot_positions(routes_ref[...], experts)
    (a8, a9), (b8, b9) = [slot_masks(e, p, experts) for e, p in picks]
    pick8 = as_bf16(jnp.logical_or(a8, b8))
    pick9 = as_bf16(jnp.logical_or(a9, b9))
    for g in range(groups):
        columns = tokens_ref[:, g * LANES : (g + 1) * LANES]
        chosen = jnp.dot(pick8, columns, preferred_element_type=jnp.float32)
        out_ref[:, g * 8 : (g + 1) * 8, :] = chosen.reshape(experts, 8, LANES).astype(jnp.bfloat16)
        last = jnp.dot(pick9, columns, preferred_element_type=jnp.float32)
        for half in range(LANES // 128):
            ninth_ref[half, pl.ds(g, experts, stride=groups), :] = last[
                :, half * 128 : (half + 1) * 128
            ]
    whole = jnp.concatenate([ninth_ref[half] for half in range(LANES // 128)], axis=1)
    out_ref[:, 8 * groups :, :] = whole.reshape(experts, groups, LANES).astype(jnp.bfloat16)


def silu_product(tokens, gate, up):
    gated = jnp.dot(tokens, gate, preferred_element_type=jnp.float32)
    lifted = jnp.dot(tokens, up, preferred_element_type=jnp.float32)
    return (gated / (1.0 + jnp.exp(-gated)) * lifted).astype(jnp.bfloat16)


def near_kernel(
    received_ref, gain_ref, g0, u0, g1, u1, g2, u2,
    hidden_ref, tokens_ref,
    ninth_ref,
):
    sources = received_ref.shape[0]
    groups = received_ref.shape[1] // 9
    width = groups * LANES
    eights = sources * 8
    ff = g0.shape[1]
    ninth = received_ref[:, 8 * groups :, :].astype(jnp.float32).reshape(sources * groups, LANES)
    for h in range(LANES // 128):
        ninth_ref[h] = ninth[:, h * 128 : (h + 1) * 128]

    def eight_rows(g):
        block = received_ref[:, g * 8 : (g + 1) * 8, :].astype(jnp.float32)
        return block.reshape(eights, LANES)

    def ninth_rows(g):
        return jnp.concatenate(
            [ninth_ref[h, pl.ds(g, sources, stride=groups), :] for h in range(LANES // 128)], axis=1
        )

    square8 = jnp.zeros((eights, LANES), jnp.float32)
    square9 = jnp.zeros((sources, LANES), jnp.float32)
    for g in range(groups):
        x = eight_rows(g)
        square8 = square8 + x * x
        y = ninth_rows(g)
        square9 = square9 + y * y
    scale8 = lax.rsqrt(jnp.sum(square8, axis=1, keepdims=True) / width + EPSILON)
    scale9 = lax.rsqrt(jnp.sum(square9, axis=1, keepdims=True) / width + EPSILON)
    for g in range(groups):
        gain = gain_ref[:, g * LANES : (g + 1) * LANES]
        tokens_ref[:eights, g * LANES : (g + 1) * LANES] = (
            eight_rows(g) * scale8 * gain
        ).astype(jnp.bfloat16)
        tokens_ref[eights:, g * LANES : (g + 1) * LANES] = (
            ninth_rows(g) * scale9 * gain
        ).astype(jnp.bfloat16)
    for n, (gate, up) in enumerate(((g0, u0), (g1, u1), (g2, u2))):
        hidden_ref[:, n * ff : (n + 1) * ff] = silu_product(tokens_ref[...], gate[...], up[...])


def far_kernel(tokens_ref, gate, up, near_ref, d0, d1, d2, hidden_ref, sum_ref):
    hidden_ref[...] = silu_product(tokens_ref[...], gate[...], up[...])
    for g in range(d0.shape[1] // LANES):
        columns = slice(g * LANES, (g + 1) * LANES)
        down = jnp.concatenate([d[:, columns] for d in (d0, d1, d2)], axis=0)
        sum_ref[:, columns] = jnp.dot(near_ref[...], down, preferred_element_type=jnp.float32)


def down_kernel(sum_ref, far_ref, d3a, d3b, out_ref, built_ref, ninth_ref, sems):
    sources = out_ref.shape[0]
    groups = out_ref.shape[1] // 9
    eights = sources * 8
    leaving = []

    def leave(part, size):
        rows = pl.ds(part * 8, size)
        copy = pltpu.make_async_copy(
            built_ref.at[:, rows, :], out_ref.at[:, rows, :], sems.at[part]
        )
        copy.start()
        leaving.append(copy)

    for g in range(groups):
        columns = slice(g * LANES, (g + 1) * LANES)
        result = sum_ref[:, columns] + jnp.dot(
            far_ref[...],
            jnp.concatenate([d3a[:, columns], d3b[:, columns]], axis=0),
            preferred_element_type=jnp.float32,
        )
        built_ref[:, g * 8 : (g + 1) * 8, :] = (
            result[:eights].reshape(sources, 8, LANES).astype(jnp.bfloat16)
        )
        leave(g, 8)
        for h in range(LANES // 128):
            ninth_ref[h, pl.ds(g, sources, stride=groups), :] = result[
                eights:, h * 128 : (h + 1) * 128
            ]
    whole = jnp.concatenate([ninth_ref[h] for h in range(LANES // 128)], axis=1)
    built_ref[:, 8 * groups :, :] = whole.reshape(sources, groups, LANES).astype(jnp.bfloat16)
    leave(groups, groups)
    for copy in leaving:
        copy.wait()


def stack_kernel(*refs):
    rows = refs[0].shape[0]
    for n, ref in enumerate(refs[:-1]):
        refs[-1][n * rows : (n + 1) * rows, :] = ref[...]


def attention_kernel(
    place_ref, queries_ref, gate_ref, mix_ref,
    k0, k1, k2, k3, k4, k5, k6, k7,
    own_ref, right_ref, left_ref, far_ref,
    scaled_ref, sums_ref, top_ref, mixed_ref,
):
    rows = queries_ref.shape[0]
    heads = queries_ref.shape[1] // HEAD
    quarter = own_ref.shape[0]
    plane, column, core = place_ref[0], place_ref[1], place_ref[2]
    sources = ((k0, 0, 0), (k1, 1, 0), (k2, 3, 0), (k3, 2, 0), (k4, 0, 1), (k5, 1, 1), (k6, 3, 1), (k7, 2, 1))
    for h in range(heads):
        part = queries_ref[:, h * HEAD : (h + 1) * HEAD].astype(jnp.float32) * HEAD ** (-0.5)
        scaled_ref[h] = jnp.concatenate([part, jnp.zeros_like(part)], axis=1).astype(jnp.bfloat16)
    sums_ref[...] = jnp.zeros_like(sums_ref)
    top_ref[...] = jnp.full_like(top_ref, NEGATIVE)
    own_index = plane * 8 + column * 2 + core
    own_gates = gate_ref[:, pl.ds(pl.multiple_of(own_index * rows, rows), rows)]
    base = own_gates[:, 0:1]

    def fold(pairs, gates, causal):
        lane = lax.broadcasted_iota(jnp.int32, pairs.shape, 1)
        values = jnp.where(lane >= HEAD, pairs.astype(jnp.float32), 1.0).astype(jnp.bfloat16)
        scores = [
            lax.dot_general(
                scaled_ref[h], pairs, (((1,), (1,)), ((), ())), preferred_element_type=jnp.float32
            )
            * LOG2E
            - gates[h : h + 1, :] * LOG2E
            for h in range(heads)
        ]
        folded = []
        for h in range(heads):
            score = scores[h]
            if causal is not None:
                score = jnp.where(causal, score, NEGATIVE)
            old_top = top_ref[h][:, 0:1]
            new_top = jnp.maximum(old_top, jnp.max(score, axis=1, keepdims=True))
            weight = jnp.exp2(score - new_top)
            top_ref[h] = jnp.broadcast_to(new_top, top_ref.shape[1:])
            folded.append((weight.astype(jnp.bfloat16), jnp.exp2(old_top - new_top)))
        for h in range(heads):
            weight, kept = folded[h]
            sums_ref[h] = sums_ref[h] * kept + jnp.dot(
                weight, values, preferred_element_type=jnp.float32
            )

    fold(
        k0[:rows, :],
        own_gates - base,
        lax.broadcasted_iota(jnp.int32, (rows, rows), 1)
        <= lax.broadcasted_iota(jnp.int32, (rows, rows), 0),
    )

    def step(back, carry):
        at = pl.multiple_of(back * rows, rows)
        for group in range(2):
            pairs, gates = [], []
            for keys, across, other in sources[group * 4 : (group + 1) * 4]:
                index = (plane - back) * 8 + ((column + 4 - across) % 4) * 2 + (core + other) % 2
                gate = gate_ref[:, pl.ds(pl.multiple_of(index * rows, rows), rows)]
                pairs.append(keys[pl.ds(at, rows), :])
                gates.append(jnp.where(index < own_index, gate - base, -NEGATIVE))
            fold(jnp.concatenate(pairs, axis=0), jnp.concatenate(gates, axis=1), None)
        return carry

    lax.fori_loop(0, plane + 1, step, 0)
    mixed = []
    for h in range(heads):
        total = sums_ref[h]
        mixed.append(total[:, HEAD:] / total[:, 0:1])
    mixed_ref[...] = jnp.concatenate(mixed, axis=1).astype(jnp.bfloat16)
    parts = 4
    for shift, out_ref in ((0, own_ref), (1, right_ref), (3, left_ref), (2, far_ref)):
        at = pl.multiple_of(((place_ref[3] + shift) % parts) * quarter, quarter)
        out_ref[...] = jnp.dot(
            mixed_ref[pl.ds(at, quarter), :], mix_ref[...], preferred_element_type=jnp.float32
        ).astype(jnp.bfloat16)


def picks_kernel(routes_ref, weight_ref, eight_ref, ninth_ref, scale_ref):
    experts = ninth_ref.shape[2]
    tokens = routes_ref.shape[1]
    row = lax.broadcasted_iota(jnp.int32, (tokens, tokens), 0)
    col = lax.broadcasted_iota(jnp.int32, (tokens, tokens), 1)

    def upright(lanes):
        return jnp.sum(jnp.where(row == col, lanes, 0.0), axis=1, keepdims=True)

    for k, (expert, place) in enumerate(slot_positions(routes_ref[...], experts)):
        expert = upright(expert.astype(jnp.float32)).astype(jnp.int32)
        place = upright(place.astype(jnp.float32)).astype(jnp.int32)
        eight = lax.broadcasted_iota(jnp.int32, (tokens, experts * 8), 1)
        ninth = lax.broadcasted_iota(jnp.int32, (tokens, experts), 1)
        eight_ref[k] = as_bf16(eight == jnp.where(place < 8, expert * 8 + place, -1))
        ninth_ref[k] = as_bf16(ninth == jnp.where(place == 8, expert, -1))
        scale_ref[k] = jnp.broadcast_to(upright(weight_ref[k : k + 1, :]), scale_ref.shape[1:])


def combine_kernel(eight_ref, last_ref, scale_ref, returned_ref, out_ref, ninth_ref):
    experts = returned_ref.shape[0]
    groups = returned_ref.shape[1] // 9
    ninth = returned_ref[:, 8 * groups :, :].astype(jnp.float32).reshape(experts * groups, LANES)
    for h in range(LANES // 128):
        ninth_ref[h] = ninth[:, h * 128 : (h + 1) * 128]
    for g in range(groups):
        eight = as_rows(returned_ref[:, g * 8 : (g + 1) * 8, :])
        last = jnp.concatenate(
            [ninth_ref[h, pl.ds(g, experts, stride=groups), :] for h in range(LANES // 128)], axis=1
        ).astype(jnp.bfloat16)
        total = 0.0
        for k in range(2):
            chosen = jnp.dot(eight_ref[k], eight, preferred_element_type=jnp.float32) + jnp.dot(
                last_ref[k], last, preferred_element_type=jnp.float32
            )
            total = total + scale_ref[k][:, 0:1] * chosen
        out_ref[:, g * LANES : (g + 1) * LANES] = total.astype(jnp.bfloat16)


def rms_scale(values, gain):
    return values * lax.rsqrt(jnp.mean(values * values, axis=-1, keepdims=True) + EPSILON) * gain


VMEM = pl.BlockSpec(memory_space=pltpu.VMEM)
SMEM = pl.BlockSpec(memory_space=pltpu.SMEM)
HBM = pl.BlockSpec(memory_space=pltpu.HBM)


def on_chip(array):
    return pltpu.with_memory_space_constraint(array, pltpu.VMEM)


def kept_on_chip(shape):
    return jax.ShapeDtypeStruct(shape, jnp.bfloat16)


def shift_pairs(down, across, other):
    return [
        (z * 8 + x * 2 + c, (z + down) % 8 * 8 + (x + across) % 4 * 2 + (c + other) % 2)
        for z in range(8)
        for x in range(4)
        for c in range(2)
    ]


def body(
    queries,
    keys_values,
    log_gate_cum,
    mix_weight,
    mix_gain,
    moe_in,
    moe_gain,
    routes,
    route_weight,
    expert_gate,
    expert_up,
    expert_down,
):
    ep_count = lax.axis_size("ep")
    tp_count = lax.axis_size("tp")
    ep_index = lax.axis_index("ep")
    place = jnp.stack(
        [ep_index // 8, ep_index // 2 % 4, ep_index % 2, lax.axis_index("tp")]
    ).astype(jnp.int32)
    to_right = [(i, (i + 1) % tp_count) for i in range(tp_count)]
    to_left = [(i, (i - 1) % tp_count) for i in range(tp_count)]
    to_far = [(i, (i + 2) % tp_count) for i in range(tp_count)]
    rows_here, width = moe_in.shape
    groups = width // LANES
    slot_rows = ep_count * 9
    ff = expert_gate.shape[2]
    lane_routes, lane_weight = routes.T, route_weight.T

    gate, up, down = expert_gate[0], expert_up[0], expert_down[0]
    gate_r = lax.ppermute(gate, "tp", to_right)
    up_l = lax.ppermute(up, "tp", to_left)
    up_r = lax.ppermute(up, "tp", to_right)
    gate_l = lax.ppermute(gate, "tp", to_left)
    down_r = lax.ppermute(down, "tp", to_right)
    down_l = lax.ppermute(down, "tp", to_left)
    gate_f = lax.ppermute(gate_r, "tp", to_right)
    up_f = lax.ppermute(up_l, "tp", to_left)
    down_fa = lax.ppermute(down_r[: ff // 2], "tp", to_right)
    down_fb = lax.ppermute(down_l[ff // 2 :], "tp", to_left)

    over_planes = [keys_values] + [
        lax.ppermute(keys_values, "ep", shift_pairs(d, 0, 0)) for d in range(1, 8)
    ]
    column_keys = pl.pallas_call(
        stack_kernel,
        out_shape=jax.ShapeDtypeStruct(
            (8 * keys_values.shape[0], keys_values.shape[1]), jnp.bfloat16
        ),
        in_specs=[VMEM] * 8,
        out_specs=VMEM,
        compiler_params=pltpu.CompilerParams(vmem_limit_bytes=8 * 2**20),
        name="stack_rows",
    )(*over_planes)
    core_keys = [column_keys] + [
        lax.ppermute(column_keys, "ep", shift_pairs(0, d, 0)) for d in (1, 3, 2)
    ]
    other_keys = [
        lax.ppermute(k, "ep", shift_pairs(0, 0, 1)) for k in core_keys
    ]

    exchange_shape = kept_on_chip((ep_count, 9 * groups, LANES))
    outgoing = pl.pallas_call(
        dispatch_kernel,
        out_shape=exchange_shape,
        in_specs=[VMEM, VMEM],
        out_specs=VMEM,
        scratch_shapes=[pltpu.VMEM((LANES // 128, ep_count * groups, 128), jnp.float32)],
        compiler_params=pltpu.CompilerParams(vmem_limit_bytes=16 * 2**20),
        name="dispatch_rows",
    )(lane_routes, moe_in)
    received = lax.all_to_all(outgoing, "ep", 0, 0, tiled=True)
    near, normed = pl.pallas_call(
        near_kernel,
        out_shape=[
            kept_on_chip((slot_rows, 3 * ff)),
            kept_on_chip((slot_rows, width)),
        ],
        in_specs=[VMEM] * 8,
        out_specs=[VMEM] * 2,
        scratch_shapes=[
            pltpu.VMEM((LANES // 128, ep_count * groups, 128), jnp.float32),
        ],
        cost_estimate=pl.CostEstimate(
            flops=12 * slot_rows * width * ff, bytes_accessed=9_000_000, transcendentals=0
        ),
        compiler_params=pltpu.CompilerParams(vmem_limit_bytes=24 * 2**20),
        name="near_rows",
    )(
        on_chip(received), moe_gain.reshape(1, width),
        gate, up, *[on_chip(w) for w in (gate_r, up_r, gate_l, up_l)],
    )
    far_hidden, near_sum = pl.pallas_call(
        far_kernel,
        out_shape=[
            kept_on_chip((slot_rows, ff)),
            jax.ShapeDtypeStruct((slot_rows, width), jnp.float32),
        ],
        in_specs=[VMEM] * 7,
        out_specs=[VMEM] * 2,
        cost_estimate=pl.CostEstimate(
            flops=10 * slot_rows * width * ff, bytes_accessed=9_000_000, transcendentals=0
        ),
        compiler_params=pltpu.CompilerParams(vmem_limit_bytes=16 * 2**20),
        name="far_rows",
    )(*[on_chip(v) for v in (normed, gate_f, up_f, near, down, down_r, down_l)])
    results = pl.pallas_call(
        down_kernel,
        out_shape=exchange_shape,
        in_specs=[VMEM] * 4,
        out_specs=HBM,
        scratch_shapes=[
            pltpu.VMEM((ep_count, 9 * groups, LANES), jnp.bfloat16),
            pltpu.VMEM((LANES // 128, ep_count * groups, 128), jnp.float32),
            pltpu.SemaphoreType.DMA((groups + 1,)),
        ],
        cost_estimate=pl.CostEstimate(
            flops=2 * slot_rows * width * ff,
            bytes_accessed=8_000_000,
            transcendentals=0,
        ),
        compiler_params=pltpu.CompilerParams(vmem_limit_bytes=56 * 2**20),
        name="down_rows",
    )(
        *[
            on_chip(v)
            for v in (near_sum, far_hidden, down_fa, down_fb)
        ]
    )
    returned = lax.all_to_all(results, "ep", 0, 0, tiled=True)
    rows, head_width = queries.shape
    heads = head_width // HEAD
    quarter = rows // tp_count
    quarter_shape = jax.ShapeDtypeStruct((quarter, width), jnp.bfloat16)
    own, right, left, far = pl.pallas_call(
        attention_kernel,
        out_shape=[quarter_shape] * 4,
        in_specs=[SMEM] + [VMEM] * 11,
        out_specs=[VMEM] * 4,
        scratch_shapes=[
            pltpu.VMEM((heads, rows, 2 * HEAD), jnp.bfloat16),
            pltpu.VMEM((heads, rows, 2 * HEAD), jnp.float32),
            pltpu.VMEM((heads, rows, 128), jnp.float32),
            pltpu.VMEM((rows, head_width), jnp.bfloat16),
        ],
        cost_estimate=pl.CostEstimate(
            flops=30_000_000_000, bytes_accessed=5_000_000, transcendentals=0
        ),
        compiler_params=pltpu.CompilerParams(vmem_limit_bytes=28 * 2**20),
        name="attend_rows",
    )(place, queries, log_gate_cum, mix_weight, *[on_chip(k) for k in core_keys + other_keys])
    from_left = lax.ppermute(right, "tp", to_right)
    from_right = lax.ppermute(left, "tp", to_left)
    from_far = lax.ppermute(far, "tp", to_far)
    projected = (
        own.astype(jnp.float32)
        + from_left.astype(jnp.float32)
        + from_right.astype(jnp.float32)
        + from_far.astype(jnp.float32)
    )
    mix_result = rms_scale(projected, mix_gain).astype(jnp.bfloat16)
    masks = pl.pallas_call(
        picks_kernel,
        out_shape=[
            jax.ShapeDtypeStruct((2, rows_here, ep_count * 8), jnp.bfloat16),
            jax.ShapeDtypeStruct((2, rows_here, ep_count), jnp.bfloat16),
            jax.ShapeDtypeStruct((2, rows_here, 128), jnp.float32),
        ],
        in_specs=[VMEM] * 2,
        out_specs=[VMEM] * 3,
        compiler_params=pltpu.CompilerParams(vmem_limit_bytes=12 * 2**20),
        name="pick_masks",
    )(lane_routes, lane_weight)
    moe_result = pl.pallas_call(
        combine_kernel,
        out_shape=jax.ShapeDtypeStruct((rows_here, width), jnp.bfloat16),
        in_specs=[VMEM] * 4,
        out_specs=VMEM,
        scratch_shapes=[pltpu.VMEM((LANES // 128, ep_count * groups, 128), jnp.float32)],
        compiler_params=pltpu.CompilerParams(vmem_limit_bytes=16 * 2**20),
        name="combine_rows",
    )(*[on_chip(m) for m in masks], on_chip(returned))
    return (mix_result, moe_result)


def solution(mesh):
    in_specs = (
        P("ep", "tp"),
        P("ep", "tp"),
        P("tp", None),
        P("tp", None),
        P(),
        P(("ep", "tp"), None),
        P(),
        P(("ep", "tp"), None),
        P(("ep", "tp"), None),
        P("ep", None, "tp"),
        P("ep", None, "tp"),
        P("ep", "tp", None),
    )
    out_specs = (P(("ep", "tp"), None), P(("ep", "tp"), None))
    return jax.shard_map(body, mesh=mesh, in_specs=in_specs, out_specs=out_specs, check_vma=False)
```

```python
import jax
import jax.numpy as jnp
from jax import lax
from jax.experimental import pallas as pl
from jax.experimental.pallas import tpu as pltpu
from jax.sharding import PartitionSpec as P


HEAD = 64
EPSILON = 1e-06
NEGATIVE = -1e30
LANES = 256
LOG2E = 1.4426950408889634


def slot_positions(routes, experts):
    tokens = routes.shape[1]
    first, second = routes[0:1, :], routes[1:2, :]
    expert_ids = lax.broadcasted_iota(jnp.int32, (experts, tokens), 0)
    one_first = (first == expert_ids).astype(jnp.float32)
    one_second = (second == expert_ids).astype(jnp.float32)
    row = lax.broadcasted_iota(jnp.int32, (tokens, tokens), 0)
    col = lax.broadcasted_iota(jnp.int32, (tokens, tokens), 1)
    earlier = (row < col).astype(jnp.float32).astype(jnp.bfloat16)
    count_first = jnp.dot(
        one_first.astype(jnp.bfloat16), earlier, preferred_element_type=jnp.float32
    )
    count_second = jnp.dot(
        one_second.astype(jnp.bfloat16), earlier, preferred_element_type=jnp.float32
    ) + jnp.sum(one_first, axis=1, keepdims=True)
    place_first = jnp.sum(one_first * count_first, axis=0, keepdims=True).astype(jnp.int32)
    place_second = jnp.sum(one_second * count_second, axis=0, keepdims=True).astype(jnp.int32)
    return (first, place_first), (second, place_second)


def slot_masks(expert, place, experts):
    tokens = expert.shape[1]
    eight = lax.broadcasted_iota(jnp.int32, (experts * 8, tokens), 0)
    ninth = lax.broadcasted_iota(jnp.int32, (experts, tokens), 0)
    in_eight = eight == jnp.where(place < 8, expert * 8 + place, -1)
    in_ninth = ninth == jnp.where(place == 8, expert, -1)
    return in_eight, in_ninth


def as_bf16(mask):
    return mask.astype(jnp.float32).astype(jnp.bfloat16)


def as_rows(block):
    wide = block.astype(jnp.float32)
    return wide.reshape(-1, block.shape[-1]).astype(jnp.bfloat16)


def dispatch_kernel(routes_ref, tokens_ref, out_ref, ninth_ref):
    experts = out_ref.shape[0]
    groups = tokens_ref.shape[1] // LANES
    picks = slot_positions(routes_ref[...], experts)
    (a8, a9), (b8, b9) = [slot_masks(e, p, experts) for e, p in picks]
    pick8 = as_bf16(jnp.logical_or(a8, b8))
    pick9 = as_bf16(jnp.logical_or(a9, b9))
    for g in range(groups):
        columns = tokens_ref[:, g * LANES : (g + 1) * LANES]
        chosen = jnp.dot(pick8, columns, preferred_element_type=jnp.float32)
        out_ref[:, g * 8 : (g + 1) * 8, :] = chosen.reshape(experts, 8, LANES).astype(jnp.bfloat16)
        last = jnp.dot(pick9, columns, preferred_element_type=jnp.float32)
        for half in range(LANES // 128):
            ninth_ref[half, pl.ds(g, experts, stride=groups), :] = last[
                :, half * 128 : (half + 1) * 128
            ]
    whole = jnp.concatenate([ninth_ref[half] for half in range(LANES // 128)], axis=1)
    out_ref[:, 8 * groups :, :] = whole.reshape(experts, groups, LANES).astype(jnp.bfloat16)


def silu_product(tokens, gate, up):
    gated = jnp.dot(tokens, gate, preferred_element_type=jnp.float32)
    lifted = jnp.dot(tokens, up, preferred_element_type=jnp.float32)
    return (gated / (1.0 + jnp.exp(-gated)) * lifted).astype(jnp.bfloat16)


def near_kernel(
    received_ref, gain_ref, g0, u0, g1, u1, g2, u2,
    hidden_ref, tokens_ref,
    ninth_ref,
):
    sources = received_ref.shape[0]
    groups = received_ref.shape[1] // 9
    width = groups * LANES
    eights = sources * 8
    ff = g0.shape[1]
    ninth = received_ref[:, 8 * groups :, :].astype(jnp.float32).reshape(sources * groups, LANES)
    for h in range(LANES // 128):
        ninth_ref[h] = ninth[:, h * 128 : (h + 1) * 128]

    def eight_rows(g):
        block = received_ref[:, g * 8 : (g + 1) * 8, :].astype(jnp.float32)
        return block.reshape(eights, LANES)

    def ninth_rows(g):
        return jnp.concatenate(
            [ninth_ref[h, pl.ds(g, sources, stride=groups), :] for h in range(LANES // 128)], axis=1
        )

    square8 = jnp.zeros((eights, LANES), jnp.float32)
    square9 = jnp.zeros((sources, LANES), jnp.float32)
    for g in range(groups):
        x = eight_rows(g)
        square8 = square8 + x * x
        y = ninth_rows(g)
        square9 = square9 + y * y
    scale8 = lax.rsqrt(jnp.sum(square8, axis=1, keepdims=True) / width + EPSILON)
    scale9 = lax.rsqrt(jnp.sum(square9, axis=1, keepdims=True) / width + EPSILON)
    for g in range(groups):
        gain = gain_ref[:, g * LANES : (g + 1) * LANES]
        tokens_ref[:eights, g * LANES : (g + 1) * LANES] = (
            eight_rows(g) * scale8 * gain
        ).astype(jnp.bfloat16)
        tokens_ref[eights:, g * LANES : (g + 1) * LANES] = (
            ninth_rows(g) * scale9 * gain
        ).astype(jnp.bfloat16)
    for n, (gate, up) in enumerate(((g0, u0), (g1, u1), (g2, u2))):
        hidden_ref[:, n * ff : (n + 1) * ff] = silu_product(tokens_ref[...], gate[...], up[...])


def far_kernel(tokens_ref, gate, up, near_ref, d0, d1, d2, hidden_ref, sum_ref):
    hidden_ref[...] = silu_product(tokens_ref[...], gate[...], up[...])
    for g in range(d0.shape[1] // LANES):
        columns = slice(g * LANES, (g + 1) * LANES)
        down = jnp.concatenate([d[:, columns] for d in (d0, d1, d2)], axis=0)
        sum_ref[:, columns] = jnp.dot(near_ref[...], down, preferred_element_type=jnp.float32)


def down_kernel(sum_ref, far_ref, d3a, d3b, out_ref, built_ref, ninth_ref, sems):
    sources = out_ref.shape[0]
    groups = out_ref.shape[1] // 9
    eights = sources * 8
    leaving = []

    def leave(part, size):
        rows = pl.ds(part * 8, size)
        copy = pltpu.make_async_copy(
            built_ref.at[:, rows, :], out_ref.at[:, rows, :], sems.at[part]
        )
        copy.start()
        leaving.append(copy)

    for g in range(groups):
        columns = slice(g * LANES, (g + 1) * LANES)
        result = sum_ref[:, columns] + jnp.dot(
            far_ref[...],
            jnp.concatenate([d3a[:, columns], d3b[:, columns]], axis=0),
            preferred_element_type=jnp.float32,
        )
        built_ref[:, g * 8 : (g + 1) * 8, :] = (
            result[:eights].reshape(sources, 8, LANES).astype(jnp.bfloat16)
        )
        leave(g, 8)
        for h in range(LANES // 128):
            ninth_ref[h, pl.ds(g, sources, stride=groups), :] = result[
                eights:, h * 128 : (h + 1) * 128
            ]
    whole = jnp.concatenate([ninth_ref[h] for h in range(LANES // 128)], axis=1)
    built_ref[:, 8 * groups :, :] = whole.reshape(sources, groups, LANES).astype(jnp.bfloat16)
    leave(groups, groups)
    for copy in leaving:
        copy.wait()


def stack_kernel(*refs):
    rows = refs[0].shape[0]
    for n, ref in enumerate(refs[:-1]):
        refs[-1][n * rows : (n + 1) * rows, :] = ref[...]


def attention_kernel(
    place_ref, queries_ref, gate_ref, mix_ref,
    k0, k1, k2, k3, k4, k5, k6, k7,
    own_ref, right_ref, left_ref, far_ref,
    scaled_ref, sums_ref, top_ref, mixed_ref,
):
    rows = queries_ref.shape[0]
    heads = queries_ref.shape[1] // HEAD
    quarter = own_ref.shape[0]
    plane, column, core = place_ref[0], place_ref[1], place_ref[2]
    sources = ((k0, 0, 0), (k1, 1, 0), (k2, 3, 0), (k3, 2, 0), (k4, 0, 1), (k5, 1, 1), (k6, 3, 1), (k7, 2, 1))
    for h in range(heads):
        part = queries_ref[:, h * HEAD : (h + 1) * HEAD].astype(jnp.float32) * HEAD ** (-0.5)
        scaled_ref[h] = jnp.concatenate([part, jnp.zeros_like(part)], axis=1).astype(jnp.bfloat16)
    sums_ref[...] = jnp.zeros_like(sums_ref)
    top_ref[...] = jnp.full_like(top_ref, NEGATIVE)
    own_index = plane * 8 + column * 2 + core
    own_gates = gate_ref[:, pl.ds(pl.multiple_of(own_index * rows, rows), rows)]
    base = own_gates[:, 0:1]

    def fold(pairs, gates, causal):
        lane = lax.broadcasted_iota(jnp.int32, pairs.shape, 1)
        values = jnp.where(lane >= HEAD, pairs.astype(jnp.float32), 1.0).astype(jnp.bfloat16)
        scores = [
            lax.dot_general(
                scaled_ref[h], pairs, (((1,), (1,)), ((), ())), preferred_element_type=jnp.float32
            )
            * LOG2E
            - gates[h : h + 1, :] * LOG2E
            for h in range(heads)
        ]
        folded = []
        for h in range(heads):
            score = scores[h]
            if causal is not None:
                score = jnp.where(causal, score, NEGATIVE)
            old_top = top_ref[h][:, 0:1]
            new_top = jnp.maximum(old_top, jnp.max(score, axis=1, keepdims=True))
            weight = jnp.exp2(score - new_top)
            top_ref[h] = jnp.broadcast_to(new_top, top_ref.shape[1:])
            folded.append((weight.astype(jnp.bfloat16), jnp.exp2(old_top - new_top)))
        for h in range(heads):
            weight, kept = folded[h]
            sums_ref[h] = sums_ref[h] * kept + jnp.dot(
                weight, values, preferred_element_type=jnp.float32
            )

    fold(
        k0[:rows, :],
        own_gates - base,
        lax.broadcasted_iota(jnp.int32, (rows, rows), 1)
        <= lax.broadcasted_iota(jnp.int32, (rows, rows), 0),
    )

    def step(back, carry):
        at = pl.multiple_of(back * rows, rows)
        for group in range(2):
            pairs, gates = [], []
            for keys, across, other in sources[group * 4 : (group + 1) * 4]:
                index = (plane - back) * 8 + ((column + 4 - across) % 4) * 2 + (core + other) % 2
                gate = gate_ref[:, pl.ds(pl.multiple_of(index * rows, rows), rows)]
                pairs.append(keys[pl.ds(at, rows), :])
                gates.append(jnp.where(index < own_index, gate - base, -NEGATIVE))
            fold(jnp.concatenate(pairs, axis=0), jnp.concatenate(gates, axis=1), None)
        return carry

    lax.fori_loop(0, plane + 1, step, 0)
    mixed = []
    for h in range(heads):
        total = sums_ref[h]
        mixed.append(total[:, HEAD:] / total[:, 0:1])
    mixed_ref[...] = jnp.concatenate(mixed, axis=1).astype(jnp.bfloat16)
    parts = 4
    for shift, out_ref in ((0, own_ref), (1, right_ref), (3, left_ref), (2, far_ref)):
        at = pl.multiple_of(((place_ref[3] + shift) % parts) * quarter, quarter)
        out_ref[...] = jnp.dot(
            mixed_ref[pl.ds(at, quarter), :], mix_ref[...], preferred_element_type=jnp.float32
        ).astype(jnp.bfloat16)


def picks_kernel(routes_ref, weight_ref, eight_ref, ninth_ref, scale_ref):
    experts = ninth_ref.shape[1]
    tokens = routes_ref.shape[1]
    row = lax.broadcasted_iota(jnp.int32, (tokens, tokens), 0)
    col = lax.broadcasted_iota(jnp.int32, (tokens, tokens), 1)

    def upright(lanes):
        return jnp.sum(jnp.where(row == col, lanes, 0.0), axis=1, keepdims=True)

    for k, (expert, place) in enumerate(slot_positions(routes_ref[...], experts)):
        expert = upright(expert.astype(jnp.float32)).astype(jnp.int32)
        place = upright(place.astype(jnp.float32)).astype(jnp.int32)
        eight = lax.broadcasted_iota(jnp.int32, (tokens, experts * 8), 1)
        ninth = lax.broadcasted_iota(jnp.int32, (tokens, experts), 1)
        rows = slice(k * tokens, (k + 1) * tokens)
        eight_ref[rows, :] = as_bf16(eight == jnp.where(place < 8, expert * 8 + place, -1))
        ninth_ref[rows, :] = as_bf16(ninth == jnp.where(place == 8, expert, -1))
        scale_ref[rows, :] = jnp.broadcast_to(
            upright(weight_ref[k : k + 1, :]), (tokens, scale_ref.shape[1])
        )


def combine_kernel(
    eight_ref, last_ref, scale_ref, returned_ref, out_ref, built_ref, ninth_ref, sems
):
    experts = returned_ref.shape[0]
    groups = returned_ref.shape[1] // 9
    tokens = out_ref.shape[0]
    ninth = returned_ref[:, 8 * groups :, :].astype(jnp.float32).reshape(experts * groups, LANES)
    for h in range(LANES // 128):
        ninth_ref[h] = ninth[:, h * 128 : (h + 1) * 128]
    leaving = []
    for g in range(groups):
        eight = as_rows(returned_ref[:, g * 8 : (g + 1) * 8, :])
        last = jnp.concatenate(
            [ninth_ref[h, pl.ds(g, experts, stride=groups), :] for h in range(LANES // 128)], axis=1
        ).astype(jnp.bfloat16)
        chosen = jnp.dot(eight_ref[...], eight, preferred_element_type=jnp.float32) + jnp.dot(
            last_ref[...], last, preferred_element_type=jnp.float32
        )
        scaled = scale_ref[:, 0:1] * chosen
        columns = pl.ds(g * LANES, LANES)
        built_ref[:, g * LANES : (g + 1) * LANES] = (scaled[:tokens] + scaled[tokens:]).astype(
            jnp.bfloat16
        )
        copy = pltpu.make_async_copy(
            built_ref.at[:, columns], out_ref.at[:, columns], sems.at[g]
        )
        copy.start()
        leaving.append(copy)
    for copy in leaving:
        copy.wait()


def rms_scale(values, gain):
    return values * lax.rsqrt(jnp.mean(values * values, axis=-1, keepdims=True) + EPSILON) * gain


VMEM = pl.BlockSpec(memory_space=pltpu.VMEM)
SMEM = pl.BlockSpec(memory_space=pltpu.SMEM)
HBM = pl.BlockSpec(memory_space=pltpu.HBM)


def on_chip(array):
    return pltpu.with_memory_space_constraint(array, pltpu.VMEM)


def kept_on_chip(shape):
    return jax.ShapeDtypeStruct(shape, jnp.bfloat16)


def shift_pairs(down, across, other):
    return [
        (z * 8 + x * 2 + c, (z + down) % 8 * 8 + (x + across) % 4 * 2 + (c + other) % 2)
        for z in range(8)
        for x in range(4)
        for c in range(2)
    ]


def body(
    queries,
    keys_values,
    log_gate_cum,
    mix_weight,
    mix_gain,
    moe_in,
    moe_gain,
    routes,
    route_weight,
    expert_gate,
    expert_up,
    expert_down,
):
    ep_count = lax.axis_size("ep")
    tp_count = lax.axis_size("tp")
    ep_index = lax.axis_index("ep")
    place = jnp.stack(
        [ep_index // 8, ep_index // 2 % 4, ep_index % 2, lax.axis_index("tp")]
    ).astype(jnp.int32)
    to_right = [(i, (i + 1) % tp_count) for i in range(tp_count)]
    to_left = [(i, (i - 1) % tp_count) for i in range(tp_count)]
    to_far = [(i, (i + 2) % tp_count) for i in range(tp_count)]
    rows_here, width = moe_in.shape
    groups = width // LANES
    slot_rows = ep_count * 9
    ff = expert_gate.shape[2]
    lane_routes, lane_weight = routes.T, route_weight.T

    gate, up, down = expert_gate[0], expert_up[0], expert_down[0]
    gate_r = lax.ppermute(gate, "tp", to_right)
    up_l = lax.ppermute(up, "tp", to_left)
    up_r = lax.ppermute(up, "tp", to_right)
    gate_l = lax.ppermute(gate, "tp", to_left)
    down_r = lax.ppermute(down, "tp", to_right)
    down_l = lax.ppermute(down, "tp", to_left)
    gate_f = lax.ppermute(gate_r, "tp", to_right)
    up_f = lax.ppermute(up_l, "tp", to_left)
    down_fa = lax.ppermute(down_r[: ff // 2], "tp", to_right)
    down_fb = lax.ppermute(down_l[ff // 2 :], "tp", to_left)

    over_planes = [keys_values] + [
        lax.ppermute(keys_values, "ep", shift_pairs(d, 0, 0)) for d in range(1, 8)
    ]
    column_keys = pl.pallas_call(
        stack_kernel,
        out_shape=jax.ShapeDtypeStruct(
            (8 * keys_values.shape[0], keys_values.shape[1]), jnp.bfloat16
        ),
        in_specs=[VMEM] * 8,
        out_specs=VMEM,
        compiler_params=pltpu.CompilerParams(vmem_limit_bytes=8 * 2**20),
        name="stack_rows",
    )(*over_planes)
    core_keys = [column_keys] + [
        lax.ppermute(column_keys, "ep", shift_pairs(0, d, 0)) for d in (1, 3, 2)
    ]
    other_keys = [
        lax.ppermute(k, "ep", shift_pairs(0, 0, 1)) for k in core_keys
    ]

    exchange_shape = kept_on_chip((ep_count, 9 * groups, LANES))
    outgoing = pl.pallas_call(
        dispatch_kernel,
        out_shape=exchange_shape,
        in_specs=[VMEM, VMEM],
        out_specs=VMEM,
        scratch_shapes=[pltpu.VMEM((LANES // 128, ep_count * groups, 128), jnp.float32)],
        compiler_params=pltpu.CompilerParams(vmem_limit_bytes=16 * 2**20),
        name="dispatch_rows",
    )(lane_routes, moe_in)
    received = lax.all_to_all(outgoing, "ep", 0, 0, tiled=True)
    near, normed = pl.pallas_call(
        near_kernel,
        out_shape=[
            kept_on_chip((slot_rows, 3 * ff)),
            kept_on_chip((slot_rows, width)),
        ],
        in_specs=[VMEM] * 8,
        out_specs=[VMEM] * 2,
        scratch_shapes=[
            pltpu.VMEM((LANES // 128, ep_count * groups, 128), jnp.float32),
        ],
        cost_estimate=pl.CostEstimate(
            flops=12 * slot_rows * width * ff, bytes_accessed=9_000_000, transcendentals=0
        ),
        compiler_params=pltpu.CompilerParams(vmem_limit_bytes=24 * 2**20),
        name="near_rows",
    )(
        on_chip(received), moe_gain.reshape(1, width),
        gate, up, *[on_chip(w) for w in (gate_r, up_r, gate_l, up_l)],
    )
    far_hidden, near_sum = pl.pallas_call(
        far_kernel,
        out_shape=[
            kept_on_chip((slot_rows, ff)),
            jax.ShapeDtypeStruct((slot_rows, width), jnp.float32),
        ],
        in_specs=[VMEM] * 7,
        out_specs=[VMEM] * 2,
        cost_estimate=pl.CostEstimate(
            flops=10 * slot_rows * width * ff, bytes_accessed=9_000_000, transcendentals=0
        ),
        compiler_params=pltpu.CompilerParams(vmem_limit_bytes=16 * 2**20),
        name="far_rows",
    )(*[on_chip(v) for v in (normed, gate_f, up_f, near, down, down_r, down_l)])
    results = pl.pallas_call(
        down_kernel,
        out_shape=exchange_shape,
        in_specs=[VMEM] * 4,
        out_specs=HBM,
        scratch_shapes=[
            pltpu.VMEM((ep_count, 9 * groups, LANES), jnp.bfloat16),
            pltpu.VMEM((LANES // 128, ep_count * groups, 128), jnp.float32),
            pltpu.SemaphoreType.DMA((groups + 1,)),
        ],
        cost_estimate=pl.CostEstimate(
            flops=2 * slot_rows * width * ff,
            bytes_accessed=8_000_000,
            transcendentals=0,
        ),
        compiler_params=pltpu.CompilerParams(vmem_limit_bytes=56 * 2**20),
        name="down_rows",
    )(
        *[
            on_chip(v)
            for v in (near_sum, far_hidden, down_fa, down_fb)
        ]
    )
    returned = lax.all_to_all(results, "ep", 0, 0, tiled=True)
    rows, head_width = queries.shape
    heads = head_width // HEAD
    quarter = rows // tp_count
    quarter_shape = jax.ShapeDtypeStruct((quarter, width), jnp.bfloat16)
    own, right, left, far = pl.pallas_call(
        attention_kernel,
        out_shape=[quarter_shape] * 4,
        in_specs=[SMEM] + [VMEM] * 11,
        out_specs=[VMEM] * 4,
        scratch_shapes=[
            pltpu.VMEM((heads, rows, 2 * HEAD), jnp.bfloat16),
            pltpu.VMEM((heads, rows, 2 * HEAD), jnp.float32),
            pltpu.VMEM((heads, rows, 128), jnp.float32),
            pltpu.VMEM((rows, head_width), jnp.bfloat16),
        ],
        cost_estimate=pl.CostEstimate(
            flops=30_000_000_000, bytes_accessed=5_000_000, transcendentals=0
        ),
        compiler_params=pltpu.CompilerParams(vmem_limit_bytes=28 * 2**20),
        name="attend_rows",
    )(place, queries, log_gate_cum, mix_weight, *[on_chip(k) for k in core_keys + other_keys])
    from_left = lax.ppermute(right, "tp", to_right)
    from_right = lax.ppermute(left, "tp", to_left)
    from_far = lax.ppermute(far, "tp", to_far)
    projected = (
        own.astype(jnp.float32)
        + from_left.astype(jnp.float32)
        + from_right.astype(jnp.float32)
        + from_far.astype(jnp.float32)
    )
    mix_result = rms_scale(projected, mix_gain).astype(jnp.bfloat16)
    masks = pl.pallas_call(
        picks_kernel,
        out_shape=[
            jax.ShapeDtypeStruct((2 * rows_here, ep_count * 8), jnp.bfloat16),
            jax.ShapeDtypeStruct((2 * rows_here, ep_count), jnp.bfloat16),
            jax.ShapeDtypeStruct((2 * rows_here, 128), jnp.float32),
        ],
        in_specs=[VMEM] * 2,
        out_specs=[VMEM] * 3,
        compiler_params=pltpu.CompilerParams(vmem_limit_bytes=12 * 2**20),
        name="pick_masks",
    )(lane_routes, lane_weight)
    moe_result = pl.pallas_call(
        combine_kernel,
        out_shape=jax.ShapeDtypeStruct((rows_here, width), jnp.bfloat16),
        in_specs=[VMEM] * 4,
        out_specs=HBM,
        scratch_shapes=[
            pltpu.VMEM((rows_here, width), jnp.bfloat16),
            pltpu.VMEM((LANES // 128, ep_count * groups, 128), jnp.float32),
            pltpu.SemaphoreType.DMA((groups,)),
        ],
        compiler_params=pltpu.CompilerParams(vmem_limit_bytes=16 * 2**20),
        name="combine_rows",
    )(*[on_chip(m) for m in masks], on_chip(returned))
    return (mix_result, moe_result)


def solution(mesh):
    in_specs = (
        P("ep", "tp"),
        P("ep", "tp"),
        P("tp", None),
        P("tp", None),
        P(),
        P(("ep", "tp"), None),
        P(),
        P(("ep", "tp"), None),
        P(("ep", "tp"), None),
        P("ep", None, "tp"),
        P("ep", None, "tp"),
        P("ep", "tp", None),
    )
    out_specs = (P(("ep", "tp"), None), P(("ep", "tp"), None))
    return jax.shard_map(body, mesh=mesh, in_specs=in_specs, out_specs=out_specs, check_vma=False)
```
